256 devices in a mesh: sp: 16 (over y, x), dp: 16 (over z, core).
Axes of the slice: x: 4, y: 4, z: 8, core: 2. Of those that a mesh axis runs over, the one named last changes fastest.
Arguments:
- tokens: bfloat16 [16, 3072, 4096], P('dp', 'sp'), may hold values from -30 to 30
- query_weight: bfloat16 [4096, 2048], P('dp', 'sp'), may hold values from -0.09375 to 0.09375
- key_weight: bfloat16 [4096, 2048], P('dp', 'sp'), may hold values from -0.09375 to 0.09375
- value_weight: bfloat16 [4096, 2048], P('dp', 'sp'), may hold values from -0.09375 to 0.09375
- cum_gate: float32 [16, 16, 3072], P('dp', 'sp'), may hold values from -12288 to 0, as said below
Outputs:
- attended: bfloat16 [16, 3072, 2048], P('dp', 'sp')
The draws below stay inside these ranges and needn't reach their ends.
Inputs may be any that keep to these rules, and one draw needn't show every extreme that they name: `cum_gate`: never rising along positions; the first position holds one step's log gate.
All inputs are finite; a program needn't handle non-finite values.
Results may differ from the reference program's by a relative error of at most 0.0076.
The reference program's roundings to bfloat16 on the way count: a program that leaves them out, or rounds other values in their place, can miss the bound.
Values may be sent and summed in bfloat16 or wider, within the bound.
A program may use at most 128 MiB of HBM per device.

```python
import jax
import jax.numpy as jnp
from jax import lax

D = 4096
HEAD = 128
TOK_DEV = 192
HEADS = 16
WIDTH = 2048
LEN = 3072
SEQS = 16


def draw_tokens(key, part):
    base = jnp.clip(jax.random.normal(jax.random.fold_in(key, 11), (SEQS, LEN, D), jnp.float32), -6.0, 6.0)
    return base.astype(jnp.bfloat16)


def shared_matrix(key):
    return jax.random.normal(jax.random.fold_in(key, 21), (D, WIDTH), jnp.float32)


def draw_query_weight(key, part):
    return (jnp.clip(shared_matrix(key), -6.0, 6.0) / 64.0).astype(jnp.bfloat16)


def draw_key_weight(key, part):
    other = jax.random.normal(jax.random.fold_in(key, 22), (D, WIDTH), jnp.float32)
    return (jnp.clip(other, -6.0, 6.0) / 64.0).astype(jnp.bfloat16)


def draw_cum_gate(key, part):
    order = jax.random.permutation(jax.random.fold_in(key, 31), HEADS)
    slow = order < HEADS // 2
    rate = jnp.where(slow, 1.0 / LEN, 1.0 / 40.0)
    blocks = LEN // TOK_DEV
    block_factor = jnp.exp(jax.random.uniform(jax.random.fold_in(key, 32), (SEQS, HEADS, blocks, 1), jnp.float32, -0.69, 0.69))
    block_factor = jnp.broadcast_to(block_factor, (SEQS, HEADS, blocks, TOK_DEV)).reshape(SEQS, HEADS, LEN)
    step_factor = jax.random.uniform(jax.random.fold_in(key, 33), (SEQS, HEADS, LEN), jnp.float32, 0.2, 1.8)
    log_gate = -rate[None, :, None] * block_factor * step_factor
    return jnp.cumsum(log_gate, axis=2).astype(jnp.float32)


def block_scale(own_key, shape, shards, least, top_value):
    gain = 1.0
    for axis_at, shards_of in shards:
        steps = jax.random.uniform(jax.random.fold_in(jax.random.fold_in(own_key, 6), axis_at), (shards_of,), jnp.float32, least / len(shards), top_value / len(shards))
        gain = gain * jnp.repeat(jnp.exp(steps), shape[axis_at] // shards_of).reshape((-1,) + (1,) * (len(shape) - 1 - axis_at))
    return gain


def centred(key, shape, deviation, bound, cuts=(), dtype=jnp.bfloat16):
    values = deviation * jax.random.normal(key, shape, jnp.float32)
    if cuts:
        values = values * block_scale(key, shape, cuts, -0.22, 0.18)
    return jnp.clip(values, -bound, bound).astype(dtype)


def setup_inputs(seed: int = 0) -> dict:
    seeds = jax.random.split(jax.random.key(seed), 6)
    tokens = draw_tokens(jax.random.fold_in(seeds[5], 71), 0)
    query_weight = draw_query_weight(jax.random.fold_in(seeds[5], 71), 0)
    key_weight = draw_key_weight(jax.random.fold_in(seeds[5], 71), 0)
    value_weight = centred(seeds[3], (D, WIDTH), D ** -0.5, 0.09375, ((0, 16), (1, 16)))
    cum_gate = draw_cum_gate(jax.random.fold_in(seeds[5], 71), 0)
    return {"tokens": tokens, "query_weight": query_weight, "key_weight": key_weight, "value_weight": value_weight, "cum_gate": cum_gate}


block_rows = 512


def attend(queries, keys, values, gates):
    length = queries.shape[0]
    scale = queries.shape[1] ** -0.5
    pieces = []
    for start in range(0, length, block_rows):
        finish = min(start + block_rows, length)
        scores = jnp.dot(queries[start:finish], keys[:finish].T, preferred_element_type=jnp.float32) * scale
        scores = scores + gates[start:finish, None] - gates[None, :finish]
        rows_at = start + lax.broadcasted_iota(jnp.int32, scores.shape, 0)
        cols_at = lax.broadcasted_iota(jnp.int32, scores.shape, 1)
        scores = jnp.where(cols_at <= rows_at, scores, -1e30)
        top = jnp.max(scores, axis=1, keepdims=True)
        weights = jnp.exp(scores - top)
        total = jnp.sum(weights, axis=1, keepdims=True)
        summed = jnp.dot(weights.astype(jnp.bfloat16), values[:finish], preferred_element_type=jnp.float32)
        pieces.append((summed / total).astype(jnp.bfloat16))
    return jnp.concatenate(pieces, axis=0)


def reference(tokens, query_weight, key_weight, value_weight, cum_gate):
    def one_sequence(inputs):
        rows, gates = inputs
        queries = jnp.dot(rows, query_weight, preferred_element_type=jnp.float32).astype(jnp.bfloat16)
        keys = jnp.dot(rows, key_weight, preferred_element_type=jnp.float32).astype(jnp.bfloat16)
        values = jnp.dot(rows, value_weight, preferred_element_type=jnp.float32).astype(jnp.bfloat16)

        def by_head(array):
            return jnp.transpose(array.reshape(LEN, HEADS, HEAD), (1, 0, 2))

        heads_out = lax.map(lambda group: attend(group[0], group[1], group[2], group[3]),
                            (by_head(queries), by_head(keys), by_head(values), gates))
        return jnp.transpose(heads_out, (1, 0, 2)).reshape(LEN, HEADS * HEAD)

    return lax.map(one_sequence, (tokens, cum_gate))
```

```python
import functools
import heapq

import jax
import jax.numpy as jnp
from jax import lax
from jax.experimental import pallas as pl
from jax.experimental.pallas import tpu as pltpu
from jax.sharding import PartitionSpec as P

MESH = pl.DeviceIdType.MESH
NX, NY, NZ = 4, 4, 8
TOK, D, HEAD = 192, 4096, 128
QKV = 3 * HEAD
ROWS = 256
LEN = 3072
A_ROWS = 96
block_rows = 512

ORDER = (0, -1, 1, -2, 2, -3, 3, 4)


def weight_messages():
    a, b = A_ROWS * QKV * 2, (ROWS - A_ROWS) * QKV * 2
    m = {}
    for sign, link in ((1, "z+"), (-1, "z-")):
        for t in range(1, 5):
            half = 0.5 if t == 4 else 1.0
            m["Bz", sign, t] = (link, b * half, [("Bz", sign, t - 1)] if t > 1 else [])
    for k, off in enumerate(ORDER):
        if off == 0:
            need = []
        elif off == 4:
            need = [("Bz", 1, 4), ("Bz", -1, 4)]
        else:
            need = [("Bz", 1 if off < 0 else -1, abs(off))]
        m["By", 1, off] = ("y+", b, need)
        m["By", -1, off] = ("y-", b, need)
        m["Bf", 1, off] = ("y+", b / 2, [("By", 1, off)])
        m["Bf", -1, off] = ("y-", b / 2, [("By", -1, off)])
        m["Bd", 0, off] = ("d", b * 4, [("By", s, off) for s in (1, -1)] + [("Bf", s, off) for s in (1, -1)])
    m["Ay", 1, 0] = ("y+", a, [])
    m["Ay", -1, 0] = ("y-", a, [])
    m["Af", 1, 0] = ("y+", a / 2, [("Ay", 1, 0)])
    m["Af", -1, 0] = ("y-", a / 2, [("Ay", -1, 0)])
    first = [("Ay", 1, 0), ("Ay", -1, 0), ("Af", 1, 0), ("Af", -1, 0)]
    for sign, link in ((1, "z+"), (-1, "z-")):
        for t in range(1, 5):
            half = 0.5 if t == 4 else 1.0
            m["Az", sign, t] = (link, a * 4 * half, [("Az", sign, t - 1)] if t > 1 else first)
    for off in ORDER:
        if off == 0:
            need = first
        elif off == 4:
            need = [("Az", 1, 4), ("Az", -1, 4)]
        else:
            need = [("Az", 1 if off < 0 else -1, abs(off))]
        m["Ad", 0, off] = ("d", a * 4, need)
    return m


def token_messages():
    h = TOK * D
    return {
        ("T", 1, 0): ("x+", h, []),
        ("T", -1, 0): ("x-", h, []),
        ("T", 1, 1): ("x+", h, []),
        ("T", -1, 1): ("x-", h, []),
        ("T", 1, 2): ("x+", h, [("T", 1, 0)]),
        ("T", -1, 2): ("x-", h, [("T", -1, 0)]),
    }


def schedule(messages):
    rate = {"d": 600e3}
    free, arrive, order = {}, {}, []
    waiting = dict(messages)
    while waiting:
        ready = {}
        for name, (link, size, need) in waiting.items():
            if all(n in arrive for n in need):
                ready[name] = max([arrive[n] for n in need], default=0.0)
        name = min(ready, key=lambda n: (ready[n], list(messages).index(n)))
        link, size, need = waiting.pop(name)
        start = max(ready[name], free.get(link, 0.0))
        end = start + (size / rate["d"] if link == "d" else 2 * size / 90e3)
        free[link] = end
        arrive[name] = end + (1.0 if link == "d" else 1.8)
        order.append(name)
    return order, arrive


def report():
    m = {**weight_messages(), **token_messages()}
    order, arrive = schedule(m)
    for n in order:
        print(n, m[n][0], int(m[n][1]), round(arrive[n], 1))
    print(len(order))


def mo(v, n):
    return pl.multiple_of(v, n)


def kernel(tok, wq, wk, wv, out, w, t, p, q, relay, load_sem, send_sem, recv_sem):
    s, d = lax.axis_index("sp"), lax.axis_index("dp")
    y, x = lax.div(s, NX), lax.rem(s, NX)
    z, c = lax.div(d, 2), lax.rem(d, 2)

    def xs(i):
        return lax.rem(x + NX + i, NX)

    def ys(i):
        return lax.rem(y + NY + i, NY)

    def zs(i):
        return lax.rem(z + NZ + i, NZ)

    def dev(dx=0, dy=0, dz=0, other=False):
        return {"sp": ys(dy) * NX + xs(dx), "dp": zs(dz) * 2 + (1 - c if other else c)}

    loads = []
    for i, ref in enumerate((wq, wk, wv)):
        loads.append(pltpu.make_async_copy(
            ref, w.at[pl.ds(mo(d * ROWS, ROWS), ROWS), pl.ds(mo(y * QKV + i * HEAD, HEAD), HEAD)], load_sem.at[i]))
    loads.append(pltpu.make_async_copy(tok, t.at[x], load_sem.at[3]))
    for copy in loads:
        copy.start()

    barrier = pltpu.get_barrier_semaphore()
    greet = [dev(dx=1), dev(dx=-1), dev(dy=1), dev(dy=-1), dev(dz=1), dev(dz=-1), dev(other=True)]
    for who in greet:
        pl.semaphore_signal(barrier, inc=1, device_id=who, device_id_type=MESH)
    pl.semaphore_wait(barrier, len(greet))

    def wrect(zo, row0, rows, col=None, other=False):
        core = 1 - c if other else c
        at = pl.ds(mo((zs(zo) * 2 + core) * ROWS + row0, 16), rows)
        if col is None:
            return w.at[at]
        return w.at[at, pl.ds(mo(ys(col) * QKV, HEAD), QKV)]

    def regions(name):
        kind, sign, i = name
        row0, rows = (0, A_ROWS) if kind[0] == "A" else (A_ROWS, ROWS - A_ROWS)
        half = rows // 2
        if kind == "T":
            if i == 2:
                at = pl.ds(0 if sign == 1 else TOK // 2, TOK // 2)
                return t.at[xs(-sign), at], t.at[xs(-2 * sign), at], dev(dx=sign)
            at = pl.ds((0 if sign == 1 else TOK // 2) if i == 0 else (TOK // 2 if sign == 1 else 0), TOK // 2)
            return t.at[x, at], t.at[xs(-sign), at], dev(dx=sign)
        if kind in ("Az", "Bz"):
            col = None if kind == "Az" else 0
            if i == 4:
                row0, rows = row0 + (0 if sign == 1 else half), half
            return wrect(-sign * (i - 1), row0, rows, col), wrect(-sign * i, row0, rows, col), dev(dz=sign)
        if kind in ("Ay", "By"):
            return wrect(i, row0, rows, 0), wrect(i, row0, rows, -sign), dev(dy=sign)
        if kind in ("Af", "Bf"):
            row0, rows = row0 + (0 if sign == 1 else half), half
            return wrect(i, row0, rows, -sign), wrect(i, row0, rows, -2 * sign), dev(dy=sign)
        return wrect(i, row0, rows), wrect(i, row0, rows, other=True), dev(other=True)

    sent, arrived = [], set()
    number = {}

    def descriptor(src, dst, name, who):
        n = number.setdefault(name, len(number))
        return pltpu.make_async_remote_copy(
            src_ref=src, dst_ref=dst, send_sem=send_sem.at[n], recv_sem=recv_sem.at[n],
            device_id=who, device_id_type=MESH)

    def start(name, src, who, dst=None):
        copy = descriptor(src, src if dst is None else dst, name, who)
        copy.start()
        sent.append(copy)

    def arrival(name, where, who):
        if name not in arrived:
            arrived.add(name)
            descriptor(where, where, name, who).wait_recv()

    loaded = set()

    def load(*which):
        for i in which:
            if i not in loaded:
                loaded.add(i)
                loads[i].wait()

    messages = {**weight_messages(), **token_messages()}
    for name in schedule(messages)[0]:
        load(*((3,) if name[0] == "T" else (0, 1, 2)))
        for need in messages[name][2]:
            src, dst, who = regions(need)
            arrival(need, dst, who)
        src, dst, who = regions(name)
        start(name, src, who)
    for name in messages:
        if name[0] != "T":
            src, dst, who = regions(name)
            arrival(name, dst, who)

    def project(block):
        @pl.loop(0, NY * QKV // 256)
        def _(j):
            cols = pl.ds(mo(j * 256, 256), 256)
            p[block, :, cols] = jnp.dot(t[block], w[:, cols], preferred_element_type=jnp.float32).astype(jnp.bfloat16)

        q[y * NX + block] = p[block, :, pl.ds(mo(y * QKV, HEAD), QKV)]

    half = TOK // 2

    def exchange(n, block):
        for sign in (1, -1):
            rows = pl.ds(0 if sign == 1 else half, half)
            start(("Qr", sign, n), p.at[block, rows, pl.ds(mo(ys(2) * QKV, HEAD), QKV)], dev(dy=sign),
                  relay.at[block, 0 if sign == 1 else 1])
        for sign in (1, -1):
            start(("Qy", sign, n), p.at[block, :, pl.ds(mo(ys(sign) * QKV, HEAD), QKV)], dev(dy=sign),
                  q.at[y * NX + block])

    def forward(n, block):
        for sign in (1, -1):
            rows = pl.ds(0 if sign == 1 else half, half)
            place = relay.at[block, 0 if sign == 1 else 1]
            arrival(("Qr", sign, n), place, dev(dy=sign))
            start(("Qf", sign, n), place, dev(dy=sign), q.at[ys(-sign) * NX + block, rows])

    blocks = (xs(0), xs(-1), xs(1), xs(2))
    needs = ((), (("T", 1, 0), ("T", 1, 1)), (("T", -1, 0), ("T", -1, 1)), (("T", 1, 2), ("T", -1, 2)))
    for n, block in enumerate(blocks):
        for need in needs[n]:
            src, dst, who = regions(need)
            arrival(need, dst, who)
        project(block)
        exchange(n, block)
        if n > 0:
            forward(n - 1, blocks[n - 1])
    forward(3, blocks[3])
    for n, block in enumerate(blocks):
        for sign in (1, -1):
            rows = pl.ds(0 if sign == 1 else half, half)
            arrival(("Qy", sign, n), q.at[ys(-sign) * NX + block], dev(dy=sign))
            arrival(("Qf", sign, n), q.at[ys(-2 * sign) * NX + block, rows], dev(dy=sign))
    result = pltpu.make_async_copy(q, out, load_sem.at[4])
    result.start()
    for copy in sent:
        copy.wait_send()
    result.wait()


def attend(queries, keys, values, gates):
    length = queries.shape[0]
    scale = queries.shape[1] ** (-0.5)
    pieces = []
    for start in range(0, length, block_rows):
        finish = min(start + block_rows, length)
        scores = (
            jnp.dot(queries[start:finish], keys[:finish].T, preferred_element_type=jnp.float32)
            * scale
        )
        scores = scores + gates[start:finish, None] - gates[None, :finish]
        rows_at = start + lax.broadcasted_iota(jnp.int32, scores.shape, 0)
        cols_at = lax.broadcasted_iota(jnp.int32, scores.shape, 1)
        scores = jnp.where(cols_at <= rows_at, scores, -1e30)
        top = jnp.max(scores, axis=1, keepdims=True)
        weights = jnp.exp(scores - top)
        total = jnp.sum(weights, axis=1, keepdims=True)
        summed = jnp.dot(
            weights.astype(jnp.bfloat16), values[:finish], preferred_element_type=jnp.float32
        )
        pieces.append((summed / total).astype(jnp.bfloat16))
    return jnp.concatenate(pieces, axis=0)


def body(tokens, query_weight, key_weight, value_weight, cum_gate):
    count = len(weight_messages()) + len(token_messages()) + 24
    any_space = pl.BlockSpec(memory_space=pl.ANY)
    qkv = pl.pallas_call(
        kernel,
        out_shape=jax.ShapeDtypeStruct((NX * NY, TOK, QKV), jnp.bfloat16),
        in_specs=[any_space] * 4,
        out_specs=any_space,
        scratch_shapes=[
            pltpu.VMEM((D, NY * QKV), jnp.bfloat16),
            pltpu.VMEM((NX, TOK, D), jnp.bfloat16),
            pltpu.VMEM((NX, TOK, NY * QKV), jnp.bfloat16),
            pltpu.VMEM((NX * NY, TOK, QKV), jnp.bfloat16),
            pltpu.VMEM((NX, 2, TOK // 2, QKV), jnp.bfloat16),
            pltpu.SemaphoreType.DMA((5,)),
            pltpu.SemaphoreType.DMA((count,)),
            pltpu.SemaphoreType.DMA((count,)),
        ],
        compiler_params=pltpu.CompilerParams(
            collective_id=0, has_side_effects=True, vmem_limit_bytes=60 * 1024 * 1024
        ),
        name="gather_project",
    )(tokens[0], query_weight, key_weight, value_weight)
    qkv = qkv.reshape(LEN, QKV)
    head_out = attend(qkv[:, :HEAD], qkv[:, HEAD : 2 * HEAD], qkv[:, 2 * HEAD :], cum_gate[0, 0])
    gathered = lax.all_to_all(head_out, "sp", split_axis=0, concat_axis=1, tiled=True)
    return gathered[None]


def solution(mesh):
    in_specs = (
        P("dp", "sp", None),
        P("dp", "sp"),
        P("dp", "sp"),
        P("dp", "sp"),
        P("dp", "sp", None),
    )
    out_specs = P("dp", "sp", None)
    return jax.shard_map(body, mesh=mesh, in_specs=in_specs, out_specs=out_specs, check_vma=False)
```

```python
import functools
import heapq

import jax
import jax.numpy as jnp
from jax import lax
from jax.experimental import pallas as pl
from jax.experimental.pallas import tpu as pltpu
from jax.sharding import PartitionSpec as P

MESH = pl.DeviceIdType.MESH
NX, NY, NZ = 4, 4, 8
TOK, D, HEAD = 192, 4096, 128
QKV = 3 * HEAD
ROWS = 256
LEN = 3072
A_ROWS = 96
Q_ROWS, K_ROWS = 384, 768
LOG2E = 1.4426950408889634

ORDER = (0, -1, 1, -2, 2, -3, 3, 4)


def weight_messages():
    a, b = A_ROWS * QKV * 2, (ROWS - A_ROWS) * QKV * 2
    m = {}
    for sign, link in ((1, "z+"), (-1, "z-")):
        for t in range(1, 5):
            half = 0.5 if t == 4 else 1.0
            m["Bz", sign, t] = (link, b * half, [("Bz", sign, t - 1)] if t > 1 else [])
    for k, off in enumerate(ORDER):
        if off == 0:
            need = []
        elif off == 4:
            need = [("Bz", 1, 4), ("Bz", -1, 4)]
        else:
            need = [("Bz", 1 if off < 0 else -1, abs(off))]
        m["By", 1, off] = ("y+", b, need)
        m["By", -1, off] = ("y-", b, need)
        m["Bf", 1, off] = ("y+", b / 2, [("By", 1, off)])
        m["Bf", -1, off] = ("y-", b / 2, [("By", -1, off)])
        m["Bd", 0, off] = ("d", b * 4, [("By", s, off) for s in (1, -1)] + [("Bf", s, off) for s in (1, -1)])
    m["Ay", 1, 0] = ("y+", a, [])
    m["Ay", -1, 0] = ("y-", a, [])
    m["Af", 1, 0] = ("y+", a / 2, [("Ay", 1, 0)])
    m["Af", -1, 0] = ("y-", a / 2, [("Ay", -1, 0)])
    first = [("Ay", 1, 0), ("Ay", -1, 0), ("Af", 1, 0), ("Af", -1, 0)]
    for sign, link in ((1, "z+"), (-1, "z-")):
        for t in range(1, 5):
            half = 0.5 if t == 4 else 1.0
            m["Az", sign, t] = (link, a * 4 * half, [("Az", sign, t - 1)] if t > 1 else first)
    for off in ORDER:
        if off == 0:
            need = first
        elif off == 4:
            need = [("Az", 1, 4), ("Az", -1, 4)]
        else:
            need = [("Az", 1 if off < 0 else -1, abs(off))]
        m["Ad", 0, off] = ("d", a * 4, need)
    return m


def token_messages():
    h = TOK * D
    return {
        ("T", 1, 0): ("x+", h, []),
        ("T", -1, 0): ("x-", h, []),
        ("T", 1, 1): ("x+", h, []),
        ("T", -1, 1): ("x-", h, []),
        ("T", 1, 2): ("x+", h, [("T", 1, 0)]),
        ("T", -1, 2): ("x-", h, [("T", -1, 0)]),
    }


def schedule(messages):
    rate = {"d": 600e3}
    free, arrive, order = {}, {}, []
    waiting = dict(messages)
    while waiting:
        ready = {}
        for name, (link, size, need) in waiting.items():
            if all(n in arrive for n in need):
                ready[name] = max([arrive[n] for n in need], default=0.0)
        name = min(ready, key=lambda n: (ready[n], list(messages).index(n)))
        link, size, need = waiting.pop(name)
        start = max(ready[name], free.get(link, 0.0))
        end = start + (size / rate["d"] if link == "d" else 2 * size / 90e3)
        free[link] = end
        arrive[name] = end + (1.0 if link == "d" else 1.8)
        order.append(name)
    return order, arrive


def report():
    m = {**weight_messages(), **token_messages()}
    order, arrive = schedule(m)
    for n in order:
        print(n, m[n][0], int(m[n][1]), round(arrive[n], 1))
    print(len(order))


def mo(v, n):
    return pl.multiple_of(v, n)


def kernel(tok, wq, wk, wv, gate, out, w, t, p, q, relay, bias, scores, head_out, load_sem, send_sem, recv_sem, out_send, out_recv):
    s, d = lax.axis_index("sp"), lax.axis_index("dp")
    y, x = lax.div(s, NX), lax.rem(s, NX)
    z, c = lax.div(d, 2), lax.rem(d, 2)

    def xs(i):
        return lax.rem(x + NX + i, NX)

    def ys(i):
        return lax.rem(y + NY + i, NY)

    def zs(i):
        return lax.rem(z + NZ + i, NZ)

    def dev(dx=0, dy=0, dz=0, other=False):
        return {"sp": ys(dy) * NX + xs(dx), "dp": zs(dz) * 2 + (1 - c if other else c)}

    loads = []
    for i, ref in enumerate((wq, wk, wv)):
        loads.append(pltpu.make_async_copy(
            ref, w.at[pl.ds(mo(d * ROWS, ROWS), ROWS), pl.ds(mo(y * QKV + i * HEAD, HEAD), HEAD)], load_sem.at[i]))
    loads.append(pltpu.make_async_copy(tok, t.at[x], load_sem.at[3]))
    for copy in loads:
        copy.start()

    barrier = pltpu.get_barrier_semaphore()
    greet = [dev(dx=dx, dy=dy) for dy in range(NY) for dx in range(NX) if dx or dy]
    greet += [dev(dz=1), dev(dz=-1), dev(other=True)]
    for who in greet:
        pl.semaphore_signal(barrier, inc=1, device_id=who, device_id_type=MESH)
    pl.semaphore_wait(barrier, len(greet))

    def wrect(zo, row0, rows, col=None, other=False):
        core = 1 - c if other else c
        at = pl.ds(mo((zs(zo) * 2 + core) * ROWS + row0, 16), rows)
        if col is None:
            return w.at[at]
        return w.at[at, pl.ds(mo(ys(col) * QKV, HEAD), QKV)]

    def regions(name):
        kind, sign, i = name
        row0, rows = (0, A_ROWS) if kind[0] == "A" else (A_ROWS, ROWS - A_ROWS)
        half = rows // 2
        if kind == "T":
            if i == 2:
                at = pl.ds(0 if sign == 1 else TOK // 2, TOK // 2)
                return t.at[xs(-sign), at], t.at[xs(-2 * sign), at], dev(dx=sign)
            at = pl.ds((0 if sign == 1 else TOK // 2) if i == 0 else (TOK // 2 if sign == 1 else 0), TOK // 2)
            return t.at[x, at], t.at[xs(-sign), at], dev(dx=sign)
        if kind in ("Az", "Bz"):
            col = None if kind == "Az" else 0
            if i == 4:
                row0, rows = row0 + (0 if sign == 1 else half), half
            return wrect(-sign * (i - 1), row0, rows, col), wrect(-sign * i, row0, rows, col), dev(dz=sign)
        if kind in ("Ay", "By"):
            return wrect(i, row0, rows, 0), wrect(i, row0, rows, -sign), dev(dy=sign)
        if kind in ("Af", "Bf"):
            row0, rows = row0 + (0 if sign == 1 else half), half
            return wrect(i, row0, rows, -sign), wrect(i, row0, rows, -2 * sign), dev(dy=sign)
        return wrect(i, row0, rows), wrect(i, row0, rows, other=True), dev(other=True)

    sent, arrived = [], set()
    number = {}

    def descriptor(src, dst, name, who):
        n = number.setdefault(name, len(number))
        return pltpu.make_async_remote_copy(
            src_ref=src, dst_ref=dst, send_sem=send_sem.at[n], recv_sem=recv_sem.at[n],
            device_id=who, device_id_type=MESH)

    def start(name, src, who, dst=None):
        copy = descriptor(src, src if dst is None else dst, name, who)
        copy.start()
        sent.append(copy)

    def arrival(name, where, who):
        if name not in arrived:
            arrived.add(name)
            descriptor(where, where, name, who).wait_recv()

    loaded = set()

    def load(*which):
        for i in which:
            if i not in loaded:
                loaded.add(i)
                loads[i].wait()

    messages = {**weight_messages(), **token_messages()}
    for name in schedule(messages)[0]:
        load(*((3,) if name[0] == "T" else (0, 1, 2)))
        for need in messages[name][2]:
            src, dst, who = regions(need)
            arrival(need, dst, who)
        src, dst, who = regions(name)
        start(name, src, who)
    for name in messages:
        if name[0] != "T":
            src, dst, who = regions(name)
            arrival(name, dst, who)

    def tokens_of(row, block, at=0, count=TOK):
        return pl.ds(mo((row * NX + block) * TOK + at, 16), count)

    def project(block):
        @pl.loop(0, NY * QKV // 256)
        def _(j):
            cols = pl.ds(mo(j * 256, 256), 256)
            p[block, :, cols] = jnp.dot(t[block], w[:, cols], preferred_element_type=jnp.float32).astype(jnp.bfloat16)

        q[tokens_of(y, block)] = p[block, :, pl.ds(mo(y * QKV, HEAD), QKV)]

    half = TOK // 2

    def exchange(n, block):
        for sign in (1, -1):
            rows = pl.ds(0 if sign == 1 else half, half)
            start(("Qr", sign, n), p.at[block, rows, pl.ds(mo(ys(2) * QKV, HEAD), QKV)], dev(dy=sign),
                  relay.at[block, 0 if sign == 1 else 1])
        for sign in (1, -1):
            start(("Qy", sign, n), p.at[block, :, pl.ds(mo(ys(sign) * QKV, HEAD), QKV)], dev(dy=sign),
                  q.at[tokens_of(y, block)])

    def forward(n, block):
        for sign in (1, -1):
            place = relay.at[block, 0 if sign == 1 else 1]
            arrival(("Qr", sign, n), place, dev(dy=sign))
            start(("Qf", sign, n), place, dev(dy=sign), q.at[tokens_of(ys(-sign), block, 0 if sign == 1 else half, half)])

    blocks = (xs(0), xs(-1), xs(1), xs(2))
    needs = ((), (("T", 1, 0), ("T", 1, 1)), (("T", -1, 0), ("T", -1, 1)), (("T", 1, 2), ("T", -1, 2)))
    for n, block in enumerate(blocks):
        for need in needs[n]:
            src, dst, who = regions(need)
            arrival(need, dst, who)
        project(block)
        exchange(n, block)
        if n > 0:
            forward(n - 1, blocks[n - 1])
    forward(3, blocks[3])
    for n, block in enumerate(blocks):
        for sign in (1, -1):
            arrival(("Qy", sign, n), q.at[tokens_of(ys(-sign), block)], dev(dy=sign))
            arrival(("Qf", sign, n), q.at[tokens_of(ys(-2 * sign), block, 0 if sign == 1 else half, half)], dev(dy=sign))

    bias[...] = gate[...] * LOG2E

    def give(block):
        rows = head_out.at[pl.ds(block * TOK, TOK)]
        place = out.at[:, pl.ds(mo(s * HEAD, HEAD), HEAD)]

        @pl.when(s != block)
        def _():
            pltpu.make_async_remote_copy(
                src_ref=rows, dst_ref=place, send_sem=out_send.at[block], recv_sem=out_recv.at[s],
                device_id={"sp": block, "dp": d}, device_id_type=MESH).start()

        @pl.when(s == block)
        def _():
            pltpu.make_async_copy(rows, place, load_sem.at[4]).start()

    @pl.loop(0, LEN // Q_ROWS)
    def _(step):
        now = lax.rem(lax.div(s, 2) + step, LEN // Q_ROWS)
        for i in range(LEN // Q_ROWS):
            @pl.when(now == i)
            def _():
                attend_rows(i, q, bias, scores, head_out)
                for block in range(i * Q_ROWS // TOK, (i + 1) * Q_ROWS // TOK):
                    give(block)

    for copy in sent:
        copy.wait_send()
    for block in range(NX * NY):
        rows = head_out.at[pl.ds(block * TOK, TOK)]

        @pl.when(s != block)
        def _():
            copy = pltpu.make_async_remote_copy(
                src_ref=rows, dst_ref=out.at[:, pl.ds(block * HEAD, HEAD)], send_sem=out_send.at[block],
                recv_sem=out_recv.at[block], device_id={"sp": block, "dp": d}, device_id_type=MESH)
            copy.wait_send()
            copy.wait_recv()

        @pl.when(s == block)
        def _():
            pltpu.make_async_copy(rows, out.at[:, pl.ds(block * HEAD, HEAD)], load_sem.at[4]).wait()


def fold(a, op):
    return functools.reduce(op, [a[:, i : i + 128] for i in range(0, a.shape[1], 128)])


def attend_rows(i, q, bias, scores, head_out):
    first, last = i * Q_ROWS, (i + 1) * Q_ROWS
    queries = q[first:last, :HEAD]
    base = bias[0:1, first : first + 1]
    scale = HEAD**-0.5 * LOG2E
    cuts = [(at, min(at + K_ROWS, last)) for at in range(0, last, K_ROWS)]
    top = None
    for at, end in cuts:
        part = lax.dot_general(queries, q[at:end, HEAD : 2 * HEAD], (((1,), (1,)), ((), ())),
                               preferred_element_type=jnp.float32)
        part = part * scale + (base - bias[0:1, at:end])
        if end > first:
            rows_at = first + lax.broadcasted_iota(jnp.int32, part.shape, 0)
            cols_at = at + lax.broadcasted_iota(jnp.int32, part.shape, 1)
            part = jnp.where(cols_at <= rows_at, part, -1e30)
        scores[:, at:end] = part
        high = fold(part, jnp.maximum)
        top = high if top is None else jnp.maximum(top, high)
    top = jnp.max(top, axis=1, keepdims=True)
    total = summed = None
    for at, end in cuts:
        weights = jnp.exp2(scores[:, at:end] - top)
        low = fold(weights, jnp.add)
        part = jnp.dot(weights.astype(jnp.bfloat16), q[at:end, 2 * HEAD :], preferred_element_type=jnp.float32)
        total = low if total is None else total + low
        summed = part if summed is None else summed + part
    head_out[first:last] = (summed / jnp.sum(total, axis=1, keepdims=True)).astype(jnp.bfloat16)


def body(tokens, query_weight, key_weight, value_weight, cum_gate):
    count = len(weight_messages()) + len(token_messages()) + 24
    any_space = pl.BlockSpec(memory_space=pl.ANY)
    vmem_space = pl.BlockSpec(memory_space=pltpu.VMEM)
    attended = pl.pallas_call(
        kernel,
        out_shape=jax.ShapeDtypeStruct((TOK, NX * NY * HEAD), jnp.bfloat16),
        in_specs=[any_space] * 4 + [vmem_space],
        out_specs=any_space,
        scratch_shapes=[
            pltpu.VMEM((D, NY * QKV), jnp.bfloat16),
            pltpu.VMEM((NX, TOK, D), jnp.bfloat16),
            pltpu.VMEM((NX, TOK, NY * QKV), jnp.bfloat16),
            pltpu.VMEM((LEN, QKV), jnp.bfloat16),
            pltpu.VMEM((NX, 2, TOK // 2, QKV), jnp.bfloat16),
            pltpu.VMEM((1, LEN), jnp.float32),
            pltpu.VMEM((Q_ROWS, LEN), jnp.float32),
            pltpu.VMEM((LEN, HEAD), jnp.bfloat16),
            pltpu.SemaphoreType.DMA((5,)),
            pltpu.SemaphoreType.DMA((count,)),
            pltpu.SemaphoreType.DMA((count,)),
            pltpu.SemaphoreType.DMA((NX * NY,)),
            pltpu.SemaphoreType.DMA((NX * NY,)),
        ],
        compiler_params=pltpu.CompilerParams(
            collective_id=0, has_side_effects=True, vmem_limit_bytes=60 * 1024 * 1024
        ),
        name="mixer",
    )(tokens[0], query_weight, key_weight, value_weight, cum_gate[0])
    return attended[None]


def solution(mesh):
    in_specs = (
        P("dp", "sp", None),
        P("dp", "sp"),
        P("dp", "sp"),
        P("dp", "sp"),
        P("dp", "sp", None),
    )
    out_specs = P("dp", "sp", None)
    return jax.shard_map(body, mesh=mesh, in_specs=in_specs, out_specs=out_specs, check_vma=False)
```

```python
import functools
import heapq

import jax
import jax.numpy as jnp
from jax import lax
from jax.experimental import pallas as pl
from jax.experimental.pallas import tpu as pltpu
from jax.sharding import PartitionSpec as P

MESH = pl.DeviceIdType.MESH
NX, NY, NZ = 4, 4, 8
TOK, D, HEAD = 192, 4096, 128
QKV = 3 * HEAD
ROWS = 256
LEN = 3072
A_ROWS = 96
Q_ROWS, K_ROWS = 384, 768
LOG2E = 1.4426950408889634

ORDER = (0, -1, 1, -2, 2, -3, 3, 4)


def weight_messages():
    a, b = A_ROWS * QKV * 2, (ROWS - A_ROWS) * QKV * 2
    m = {}
    m["Ay", 1, 0] = ("y+", a, [])
    m["Ay", -1, 0] = ("y-", a, [])
    m["Af", 1, 0] = ("y+", a / 2, [("Ay", 1, 0)])
    m["Af", -1, 0] = ("y-", a / 2, [("Ay", -1, 0)])
    for sign, link in ((1, "z+"), (-1, "z-")):
        for t in range(1, 5):
            half = 0.5 if t == 4 else 1.0
            m["Bz", sign, t] = (link, b * half, [("Bz", sign, t - 1)] if t > 1 else [])
    for k, off in enumerate(ORDER):
        if off == 0:
            need = []
        elif off == 4:
            need = [("Bz", 1, 4), ("Bz", -1, 4)]
        else:
            need = [("Bz", 1 if off < 0 else -1, abs(off))]
        m["By", 1, off] = ("y+", b, need)
        m["By", -1, off] = ("y-", b, need)
        m["Bf", 1, off] = ("y+", b / 2, [("By", 1, off)])
        m["Bf", -1, off] = ("y-", b / 2, [("By", -1, off)])
        m["Bd", 0, off] = ("d", b * 4, [("By", s, off) for s in (1, -1)] + [("Bf", s, off) for s in (1, -1)])
    first = [("Ay", 1, 0), ("Ay", -1, 0), ("Af", 1, 0), ("Af", -1, 0)]
    for sign, link in ((1, "z+"), (-1, "z-")):
        for t in range(1, 5):
            half = 0.5 if t == 4 else 1.0
            m["Az", sign, t] = (link, a * 4 * half, [("Az", sign, t - 1)] if t > 1 else first)
    for off in ORDER:
        if off == 0:
            need = first
        elif off == 4:
            need = [("Az", 1, 4), ("Az", -1, 4)]
        else:
            need = [("Az", 1 if off < 0 else -1, abs(off))]
        m["Ad", 0, off] = ("d", a * 4, need)
    return m


def token_messages():
    h = TOK * D
    return {
        ("T", 1, 0): ("x+", h, []),
        ("T", -1, 0): ("x-", h, []),
        ("T", 1, 1): ("x+", h, []),
        ("T", -1, 1): ("x-", h, []),
        ("T", 1, 2): ("x+", h, [("T", 1, 0)]),
        ("T", -1, 2): ("x-", h, [("T", -1, 0)]),
    }


def schedule(messages):
    rate = {"d": 600e3}
    free, arrive, order = {}, {}, []
    waiting = dict(messages)
    while waiting:
        ready = {}
        for name, (link, size, need) in waiting.items():
            if all(n in arrive for n in need):
                ready[name] = max([arrive[n] for n in need], default=0.0)
        name = min(ready, key=lambda n: (ready[n], list(messages).index(n)))
        link, size, need = waiting.pop(name)
        start = max(ready[name], free.get(link, 0.0))
        end = start + (size / rate["d"] if link == "d" else 2 * size / 90e3)
        free[link] = end
        arrive[name] = end + (1.0 if link == "d" else 1.8)
        order.append(name)
    return order, arrive


def report():
    m = {**weight_messages(), **token_messages()}
    order, arrive = schedule(m)
    for n in order:
        print(n, m[n][0], int(m[n][1]), round(arrive[n], 1))
    print(len(order))


def mo(v, n):
    return pl.multiple_of(v, n)


def kernel(tok, wq, wk, wv, gate, out, w, t, p, q, relay, bias, scores, head_out, load_sem, send_sem, recv_sem, out_send, out_recv):
    s, d = lax.axis_index("sp"), lax.axis_index("dp")
    y, x = lax.div(s, NX), lax.rem(s, NX)
    z, c = lax.div(d, 2), lax.rem(d, 2)

    def xs(i):
        return lax.rem(x + NX + i, NX)

    def ys(i):
        return lax.rem(y + NY + i, NY)

    def zs(i):
        return lax.rem(z + NZ + i, NZ)

    def dev(dx=0, dy=0, dz=0, other=False):
        return {"sp": ys(dy) * NX + xs(dx), "dp": zs(dz) * 2 + (1 - c if other else c)}

    loads = []
    for i, ref in enumerate((wq, wk, wv)):
        loads.append(pltpu.make_async_copy(
            ref, w.at[pl.ds(mo(d * ROWS, ROWS), ROWS), pl.ds(mo(y * QKV + i * HEAD, HEAD), HEAD)], load_sem.at[i]))
    loads.append(pltpu.make_async_copy(tok, t.at[x], load_sem.at[3]))
    for copy in loads:
        copy.start()

    barrier = pltpu.get_barrier_semaphore()
    greet = [dev(dx=dx, dy=dy) for dy in range(NY) for dx in range(NX) if dx or dy]
    greet += [dev(dz=1), dev(dz=-1), dev(other=True)]
    for who in greet:
        pl.semaphore_signal(barrier, inc=1, device_id=who, device_id_type=MESH)
    pl.semaphore_wait(barrier, len(greet))

    def wrect(zo, row0, rows, col=None, other=False):
        core = 1 - c if other else c
        at = pl.ds(mo((zs(zo) * 2 + core) * ROWS + row0, 16), rows)
        if col is None:
            return w.at[at]
        return w.at[at, pl.ds(mo(ys(col) * QKV, HEAD), QKV)]

    def regions(name):
        kind, sign, i = name
        row0, rows = (0, A_ROWS) if kind[0] == "A" else (A_ROWS, ROWS - A_ROWS)
        half = rows // 2
        if kind == "T":
            if i == 2:
                at = pl.ds(0 if sign == 1 else TOK // 2, TOK // 2)
                return t.at[xs(-sign), at], t.at[xs(-2 * sign), at], dev(dx=sign)
            at = pl.ds((0 if sign == 1 else TOK // 2) if i == 0 else (TOK // 2 if sign == 1 else 0), TOK // 2)
            return t.at[x, at], t.at[xs(-sign), at], dev(dx=sign)
        if kind in ("Az", "Bz"):
            col = None if kind == "Az" else 0
            if i == 4:
                row0, rows = row0 + (0 if sign == 1 else half), half
            return wrect(-sign * (i - 1), row0, rows, col), wrect(-sign * i, row0, rows, col), dev(dz=sign)
        if kind in ("Ay", "By"):
            return wrect(i, row0, rows, 0), wrect(i, row0, rows, -sign), dev(dy=sign)
        if kind in ("Af", "Bf"):
            row0, rows = row0 + (0 if sign == 1 else half), half
            return wrect(i, row0, rows, -sign), wrect(i, row0, rows, -2 * sign), dev(dy=sign)
        return wrect(i, row0, rows), wrect(i, row0, rows, other=True), dev(other=True)

    sent, arrived = [], set()
    number = {}

    def descriptor(src, dst, name, who):
        n = number.setdefault(name, len(number))
        return pltpu.make_async_remote_copy(
            src_ref=src, dst_ref=dst, send_sem=send_sem.at[n], recv_sem=recv_sem.at[n],
            device_id=who, device_id_type=MESH)

    def start(name, src, who, dst=None):
        copy = descriptor(src, src if dst is None else dst, name, who)
        copy.start()
        sent.append(copy)

    def arrival(name, where, who):
        if name not in arrived:
            arrived.add(name)
            descriptor(where, where, name, who).wait_recv()

    loaded = set()

    def load(*which):
        for i in which:
            if i not in loaded:
                loaded.add(i)
                loads[i].wait()

    messages = {**weight_messages(), **token_messages()}
    for name in schedule(messages)[0]:
        load(*((3,) if name[0] == "T" else (0, 1, 2)))
        for need in messages[name][2]:
            src, dst, who = regions(need)
            arrival(need, dst, who)
        src, dst, who = regions(name)
        start(name, src, who)
    for name in messages:
        if name[0] != "T":
            src, dst, who = regions(name)
            arrival(name, dst, who)

    def tokens_of(row, block, at=0, count=TOK):
        return pl.ds(mo((row * NX + block) * TOK + at, 16), count)

    def project(block):
        @pl.loop(0, NY * QKV // 256)
        def _(j):
            cols = pl.ds(mo(j * 256, 256), 256)
            p[block, :, cols] = jnp.dot(t[block], w[:, cols], preferred_element_type=jnp.float32).astype(jnp.bfloat16)

        q[tokens_of(y, block)] = p[block, :, pl.ds(mo(y * QKV, HEAD), QKV)]

    half = TOK // 2

    def exchange(n, block):
        for sign in (1, -1):
            rows = pl.ds(0 if sign == 1 else half, half)
            start(("Qr", sign, n), p.at[block, rows, pl.ds(mo(ys(2) * QKV, HEAD), QKV)], dev(dy=sign),
                  relay.at[block, 0 if sign == 1 else 1])
        for sign in (1, -1):
            start(("Qy", sign, n), p.at[block, :, pl.ds(mo(ys(sign) * QKV, HEAD), QKV)], dev(dy=sign),
                  q.at[tokens_of(y, block)])

    def forward(n, block):
        for sign in (1, -1):
            place = relay.at[block, 0 if sign == 1 else 1]
            arrival(("Qr", sign, n), place, dev(dy=sign))
            start(("Qf", sign, n), place, dev(dy=sign), q.at[tokens_of(ys(-sign), block, 0 if sign == 1 else half, half)])

    blocks = (xs(0), xs(-1), xs(1), xs(2))
    needs = ((), (("T", 1, 0), ("T", 1, 1)), (("T", -1, 0), ("T", -1, 1)), (("T", 1, 2), ("T", -1, 2)))
    for n, block in enumerate(blocks):
        for need in needs[n]:
            src, dst, who = regions(need)
            arrival(need, dst, who)
        project(block)
        exchange(n, block)
        if n > 0:
            forward(n - 1, blocks[n - 1])
    forward(3, blocks[3])
    for n, block in enumerate(blocks):
        for sign in (1, -1):
            arrival(("Qy", sign, n), q.at[tokens_of(ys(-sign), block)], dev(dy=sign))
            arrival(("Qf", sign, n), q.at[tokens_of(ys(-2 * sign), block, 0 if sign == 1 else half, half)], dev(dy=sign))

    bias[...] = gate[...] * LOG2E

    def give(block):
        rows = head_out.at[pl.ds(block * TOK, TOK)]
        place = out.at[s]

        @pl.when(s != block)
        def _():
            pltpu.make_async_remote_copy(
                src_ref=rows, dst_ref=place, send_sem=out_send.at[block], recv_sem=out_recv.at[s],
                device_id={"sp": block, "dp": d}, device_id_type=MESH).start()

        @pl.when(s == block)
        def _():
            pltpu.make_async_copy(rows, place, load_sem.at[4]).start()

    @pl.loop(0, LEN // Q_ROWS)
    def _(step):
        now = lax.rem(lax.div(s, 2) + step, LEN // Q_ROWS)
        for i in range(LEN // Q_ROWS):
            @pl.when(now == i)
            def _():
                attend_rows(i, q, bias, scores, head_out)
                for block in range(i * Q_ROWS // TOK, (i + 1) * Q_ROWS // TOK):
                    give(block)

    for copy in sent:
        copy.wait_send()
    for block in range(NX * NY):
        rows = head_out.at[pl.ds(block * TOK, TOK)]

        @pl.when(s != block)
        def _():
            copy = pltpu.make_async_remote_copy(
                src_ref=rows, dst_ref=out.at[block], send_sem=out_send.at[block],
                recv_sem=out_recv.at[block], device_id={"sp": block, "dp": d}, device_id_type=MESH)
            copy.wait_send()
            copy.wait_recv()

        @pl.when(s == block)
        def _():
            pltpu.make_async_copy(rows, out.at[block], load_sem.at[4]).wait()


def fold(a, op):
    return functools.reduce(op, [a[:, i : i + 128] for i in range(0, a.shape[1], 128)])


def attend_rows(i, q, bias, scores, head_out):
    first, last = i * Q_ROWS, (i + 1) * Q_ROWS
    queries = q[first:last, :HEAD]
    base = bias[0:1, first : first + 1]
    scale = HEAD**-0.5 * LOG2E
    cuts = [(at, min(at + K_ROWS, last)) for at in range(0, last, K_ROWS)]
    top = None
    for at, end in cuts:
        part = lax.dot_general(queries, q[at:end, HEAD : 2 * HEAD], (((1,), (1,)), ((), ())),
                               preferred_element_type=jnp.float32)
        part = part * scale + (base - bias[0:1, at:end])
        if end > first:
            rows_at = first + lax.broadcasted_iota(jnp.int32, part.shape, 0)
            cols_at = at + lax.broadcasted_iota(jnp.int32, part.shape, 1)
            part = jnp.where(cols_at <= rows_at, part, -1e30)
        scores[:, at:end] = part
        high = fold(part, jnp.maximum)
        top = high if top is None else jnp.maximum(top, high)
    top = jnp.max(top, axis=1, keepdims=True)
    total = summed = None
    for at, end in cuts:
        weights = jnp.exp2(scores[:, at:end] - top)
        low = fold(weights, jnp.add)
        part = jnp.dot(weights.astype(jnp.bfloat16), q[at:end, 2 * HEAD :], preferred_element_type=jnp.float32)
        total = low if total is None else total + low
        summed = part if summed is None else summed + part
    head_out[first:last] = (summed / jnp.sum(total, axis=1, keepdims=True)).astype(jnp.bfloat16)


def merge(heads, out, held, sem):
    come = [pltpu.make_async_copy(heads.at[i], held.at[i], sem.at[0, i]) for i in range(NX * NY)]
    go = [pltpu.make_async_copy(held.at[i], out.at[:, pl.ds(i * HEAD, HEAD)], sem.at[1, i]) for i in range(NX * NY)]
    for copy in come:
        copy.start()
    for one, other in zip(come, go):
        one.wait()
        other.start()
    for copy in go:
        copy.wait()


def body(tokens, query_weight, key_weight, value_weight, cum_gate):
    count = len(weight_messages()) + len(token_messages()) + 24
    any_space = pl.BlockSpec(memory_space=pl.ANY)
    vmem_space = pl.BlockSpec(memory_space=pltpu.VMEM)
    attended = pl.pallas_call(
        kernel,
        out_shape=jax.ShapeDtypeStruct((NX * NY, TOK, HEAD), jnp.bfloat16),
        in_specs=[any_space] * 4 + [vmem_space],
        out_specs=any_space,
        scratch_shapes=[
            pltpu.VMEM((D, NY * QKV), jnp.bfloat16),
            pltpu.VMEM((NX, TOK, D), jnp.bfloat16),
            pltpu.VMEM((NX, TOK, NY * QKV), jnp.bfloat16),
            pltpu.VMEM((LEN, QKV), jnp.bfloat16),
            pltpu.VMEM((NX, 2, TOK // 2, QKV), jnp.bfloat16),
            pltpu.VMEM((1, LEN), jnp.float32),
            pltpu.VMEM((Q_ROWS, LEN), jnp.float32),
            pltpu.VMEM((LEN, HEAD), jnp.bfloat16),
            pltpu.SemaphoreType.DMA((5,)),
            pltpu.SemaphoreType.DMA((count,)),
            pltpu.SemaphoreType.DMA((count,)),
            pltpu.SemaphoreType.DMA((NX * NY,)),
            pltpu.SemaphoreType.DMA((NX * NY,)),
        ],
        compiler_params=pltpu.CompilerParams(
            collective_id=0, has_side_effects=True, vmem_limit_bytes=60 * 1024 * 1024
        ),
        name="mixer",
    )(tokens[0], query_weight, key_weight, value_weight, cum_gate[0])
    merged = pl.pallas_call(
        merge,
        out_shape=jax.ShapeDtypeStruct((TOK, NX * NY * HEAD), jnp.bfloat16),
        in_specs=[any_space],
        out_specs=any_space,
        scratch_shapes=[pltpu.VMEM((NX * NY, TOK, HEAD), jnp.bfloat16), pltpu.SemaphoreType.DMA((2, NX * NY))],
        name="merge",
    )(attended)
    return merged[None]


def solution(mesh):
    in_specs = (
        P("dp", "sp", None),
        P("dp", "sp"),
        P("dp", "sp"),
        P("dp", "sp"),
        P("dp", "sp", None),
    )
    out_specs = P("dp", "sp", None)
    return jax.shard_map(body, mesh=mesh, in_specs=in_specs, out_specs=out_specs, check_vma=False)
```

```python
import functools

import jax
import jax.numpy as jnp
from jax import lax
from jax.experimental import pallas as pl
from jax.experimental.pallas import tpu as pltpu
from jax.sharding import PartitionSpec as P

MESH = pl.DeviceIdType.MESH
NX, NY, NZ = 4, 4, 8
TOK, D, HEAD = 192, 4096, 128
HALF = TOK // 2
ROWS = 256
LEN = 3072
GROUP = NY * TOK
LOG2E = 1.4426950408889634

QKV = 3 * HEAD
A_ROWS = 96
ORDER = (0, -1, 1, -2, 2, -3, 3, 4)
OFF = (0, -1, 1, 2)
BATCHES = ((0, 1, 2), (3,))
TILE_US, PAIR_US = (1.4, 0.65), 0.9
TILES = (3, 4, 5, 2, 1, 0)


def weight_messages():
    a, b, g = A_ROWS * QKV * 2, (ROWS - A_ROWS) * QKV * 2, 0
    m = {}
    for sign, link in ((1, "y+"), (-1, "y-")):
        m["Ay", g, sign, 0] = (link, a, [])
    for sign, link in ((1, "y+"), (-1, "y-")):
        m["Af", g, sign, 0] = (link, a / 2, [("Ay", g, sign, 0)])
    first = [(kind, g, sign, 0) for kind in ("Ay", "Af") for sign in (1, -1)]

    def along_z(kind, size, need):
        for sign, link in ((1, "z+"), (-1, "z-")):
            for t in range(1, 5):
                m[kind, g, sign, t] = (link, size * (0.5 if t == 4 else 1), [(kind, g, sign, t - 1)] if t > 1 else need)

    def block(kind, off, own):
        if off == 0:
            return own
        if off == 4:
            return [(kind, g, 1, 4), (kind, g, -1, 4)]
        return [(kind, g, 1 if off < 0 else -1, abs(off))]

    if b:
        along_z("Bz", b, [])
        for off in ORDER:
            need = block("Bz", off, [])
            for sign, link in ((1, "y+"), (-1, "y-")):
                m["By", g, sign, off] = (link, b, need)
                m["Bf", g, sign, off] = (link, b / 2, [("By", g, sign, off)])
            m["Bd", g, 0, off] = ("d", b * 4, [(kind, g, sign, off) for kind in ("By", "Bf") for sign in (1, -1)])
    along_z("Az", a * 4, first)
    for off in ORDER:
        m["Ad", g, 0, off] = ("d", a * 4, block("Az", off, first))
    return m


def token_messages():
    h = HALF * D * 2
    m = {}
    for i in range(3):
        for sign, link in ((1, "x+"), (-1, "x-")):
            m["T", 0, sign, i] = (link, h, [("T", 0, sign, 0)] if i == 2 else [])
    return m


def batch_of(n):
    return next(i for i, batch in enumerate(BATCHES) if n in batch)


def exchange_messages(n):
    m = {}
    size = TOK * QKV * 2
    for sign, link in ((1, "y+"), (-1, "y-")):
        m["Er", 0, sign, n] = (link, size / 2, [("tile", batch_of(n), 3), ("tile", batch_of(n), 4)])
        m["Ef", 0, sign, n] = (link, size / 2, [("Er", 0, sign, n)])
        m["Ey", 0, sign, n] = (link, size, [("tile", batch_of(n), 5 if sign < 0 else 1)])
    return m


def tasks():
    t = {}
    tokens = ([], [("T", 0, 1, 0), ("T", 0, 1, 1)], [("T", 0, -1, 0), ("T", 0, -1, 1)], [("T", 0, 1, 2), ("T", 0, -1, 2)])
    for i, batch in enumerate(BATCHES):
        for j in TILES:
            need = [k for n in batch for k in tokens[n]] + list(weight_messages())
            t["tile", i, j] = (TILE_US[i], need)
    done = [[(kind, 0, sign, n) for kind in ("Ey", "Ef") for sign in (1, -1)] for n in range(NX)]
    last = NX - 1
    order = [(m, n) for m in range(last) for n in range(last)]
    order += [(last, n) for n in range(NX)] + [(m, last) for m in (1, 2, 0)]
    for m, n in order:
        t["pair", m, n] = (PAIR_US, done[n] + done[m])
    names = list(t)
    for before, name in zip(names, names[1:]):
        t[name][1].append(before)
    return t


def schedule():
    messages = {}
    for some in (weight_messages(), token_messages(), *(exchange_messages(n) for n in range(NX))):
        messages.update(some)
    work = tasks()
    place = {name: i for i, name in enumerate([*messages, *work])}
    done, free, order, now = {}, {}, [], 0.0
    left = dict.fromkeys(place)
    while left:
        ready = []
        for name in left:
            need = messages[name][2] if name in messages else work[name][1]
            if all(k in done for k in need):
                at = max([done[k] for k in need], default=0.0)
                ready.append((max(at, now), name in work, at if name in messages else 0.0, place[name], name))
        at, heavy, _, _, name = min(ready)
        del left[name]
        order.append(name)
        now = at
        if heavy:
            now += work[name][0]
            done[name] = now
        else:
            link, size, _ = messages[name]
            end = max(now, free.get(link, 0.0)) + (size / 600e3 if link == "d" else size / 45e3)
            free[link] = end
            done[name] = end + (1.0 if link == "d" else 1.8)
    return order, messages, work, done, free


def mo(v, n):
    return pl.multiple_of(v, n)


def fold(parts, op):
    return functools.reduce(op, parts)


def kernel(tok, wq, wk, wv, gate, out, w, t, p, relay, qkv, bias, high, total, summed, heads,
           load_sem, send_sem, recv_sem):
    s, d = lax.axis_index("sp"), lax.axis_index("dp")
    y, x = lax.div(s, NX), lax.rem(s, NX)
    z, c = lax.div(d, 2), lax.rem(d, 2)

    def xs(i):
        return lax.rem(x + NX + i, NX)

    def ys(i):
        return lax.rem(y + NY + i, NY)

    def zs(i):
        return lax.rem(z + NZ + i, NZ)

    def dev(dx=0, dy=0, dz=0, other=False):
        return {"sp": ys(dy) * NX + xs(dx), "dp": zs(dz) * 2 + (1 - c if other else c)}

    own = pl.ds(mo(d * ROWS, ROWS), ROWS)
    loads = []
    for i, (ref, at) in enumerate(((wq, 0), (wk, HEAD), (wv, 2 * HEAD))):
        loads.append(pltpu.make_async_copy(ref, w.at[own, pl.ds(at, HEAD)], load_sem.at[i]))
    loads.append(pltpu.make_async_copy(tok, t.at[0], load_sem.at[3]))
    for copy in loads:
        copy.start()

    barrier = pltpu.get_barrier_semaphore()
    greet = [dev(dx=dx, dy=dy) for dy in range(NY) for dx in range(NX) if dx or dy]
    greet += [dev(dz=1), dev(dz=-1), dev(other=True)]
    for who in greet:
        pl.semaphore_signal(barrier, inc=1, device_id=who, device_id_type=MESH)
    for b in range(NX):
        bias[b] = LOG2E * jnp.concatenate(
            [gate[0:1, (NX * i + b) * TOK : (NX * i + b + 1) * TOK] for i in range(NY)], axis=1)
    pl.semaphore_wait(barrier, len(greet))

    def wrect(zo, row0, rows, col=None, other=False):
        core = 1 - c if other else c
        at = pl.ds(mo((zs(zo) * 2 + core) * ROWS + row0, 16), rows)
        if col is None:
            return w.at[at]
        return w.at[at, pl.ds(col % NY * QKV, QKV)]

    def part(sign):
        return 0 if sign == 1 else HALF

    def seat(n, dy, at=0, count=TOK):
        return qkv.at[n, pl.ds(mo(ys(dy) * TOK + at, 16), count)]

    def regions(name):
        kind, g, sign, i = name
        if kind == "T":
            near = OFF.index(-sign)
            if i == 2:
                at = pl.ds(part(sign), HALF)
                return t.at[near, at], t.at[3, at], t.at[3, at], dev(dx=sign)
            at = pl.ds(part(sign) if i == 0 else part(-sign), HALF)
            return t.at[0, at], t.at[near, at], t.at[near, at], dev(dx=sign)
        if kind == "O":
            source = heads.at[g, pl.ds(mo(ys(sign) * TOK, 16), TOK)]
            return source, out.at[s], out.at[ys(-sign) * NX + xs(-OFF[g])], dev(dx=OFF[g], dy=sign)
        if kind[0] == "E":
            hop = relay.at[i, 0 if sign == 1 else 1]

            def stage(r, at=0, count=TOK):
                return p.at[i, pl.ds(at, count), pl.ds(r * QKV, QKV)]

            if kind == "Er":
                return stage(2, part(sign), HALF), hop, hop, dev(dy=sign)
            if kind == "Ef":
                return (hop, seat(i, -sign, part(sign), HALF), seat(i, -2 * sign, part(sign), HALF),
                        dev(dy=sign))
            return stage(sign % NY), seat(i, 0), seat(i, -sign), dev(dy=sign)
        row0, rows = (0, A_ROWS) if kind[0] == "A" else (A_ROWS, ROWS - A_ROWS)
        half = rows // 2
        if kind[1] == "z":
            col = None if kind == "Az" else 0
            if i == 4:
                row0, rows = row0 + (0 if sign == 1 else half), half
            source = wrect(-sign * (i - 1), row0, rows, col)
            return source, source, wrect(-sign * i, row0, rows, col), dev(dz=sign)
        if kind[1] == "y":
            return wrect(i, row0, rows, 0), wrect(i, row0, rows, -sign), wrect(i, row0, rows, -sign), dev(dy=sign)
        if kind[1] == "f":
            row0, rows = row0 + (0 if sign == 1 else half), half
            return wrect(i, row0, rows, -sign), wrect(i, row0, rows, 2), wrect(i, row0, rows, 2), dev(dy=sign)
        source = wrect(i, row0, rows)
        return source, source, wrect(i, row0, rows, other=True), dev(other=True)

    started, arrived, number = [], set(), {}

    def copy_of(name, source, target, who):
        n = number.setdefault(name, len(number))
        return pltpu.make_async_remote_copy(
            src_ref=source, dst_ref=target, send_sem=send_sem.at[n], recv_sem=recv_sem.at[n],
            device_id=who, device_id_type=MESH)

    def start(name):
        source, target, _, who = regions(name)
        copy_of(name, source, target, who).start()
        started.append(name)

    def arrival(name):
        if name not in arrived:
            arrived.add(name)
            _, _, where, who = regions(name)
            copy_of(name, where, where, who).wait_recv()

    order, messages, work, _, _ = schedule()
    loaded = set()

    def message(name):
        for i in (3,) if name[0] == "T" else (0, 1, 2) if name[0][0] in "AB" else ():
            if i not in loaded:
                loaded.add(i)
                loads[i].wait()
        for need in messages[name][2]:
            if need in messages:
                arrival(need)
        start(name)

    names = [name for name in order if name in work]
    ahead = {}
    waiting = []
    for name in order:
        if name in work:
            ahead[name] = waiting
            waiting = []
        else:
            waiting.append(name)

    def before(name):
        previous = names.index(name) - 1
        if previous >= 0:
            kind, i, j = names[previous]
            if kind == "tile" and j == TILES[-1]:
                for n in BATCHES[i]:
                    qkv[n, pl.ds(mo(y * TOK, TOK), TOK)] = p[n, :, :QKV]
        for item in ahead[name]:
            message(item)
        for need in work[name][1]:
            if need in messages:
                arrival(need)

    def loop(some, run, after=None):
        before(some[0])

        @pl.loop(0, len(some))
        def _(step):
            for k, name in enumerate(some):
                if k:
                    @pl.when(step == k)
                    def _():
                        before(name)
            run(step)
            for k, name in enumerate(some):
                if after and name in after:
                    @pl.when(step == k)
                    def _():
                        after[name]()

    def pick(values, step):
        value = jnp.int32(values[0])
        for k in range(1, len(values)):
            if values[k] != values[k - 1]:
                value = jnp.where(step >= k, values[k], value)
        return value

    for i, batch in enumerate(BATCHES):
        def tile(step):
            j = pick(TILES, step)
            rows = t[batch[0] : batch[-1] + 1].reshape(len(batch) * TOK, D)
            rows = jnp.dot(rows, w[:, pl.ds(mo(j * 256, 256), 256)], preferred_element_type=jnp.float32)
            rows = rows.astype(jnp.bfloat16).reshape(len(batch), TOK, 256)
            for n, block in zip(batch, rows):
                p[n, :, pl.ds(mo(j * 256, 256), 256)] = block

        loop([("tile", i, j) for j in TILES], tile)

    pairs = [name for name in names if name[0] == "pair"]
    local = pltpu.make_async_copy(heads.at[0, pl.ds(mo(y * TOK, 16), TOK)], out.at[s], load_sem.at[4])

    for m in range(NX):
        high[m] = jnp.full((GROUP, HEAD), -1e30, jnp.float32)
        total[m] = jnp.zeros((GROUP, HEAD), jnp.float32)
        summed[m] = jnp.zeros((GROUP, HEAD), jnp.float32)

    def pair(step):
        m, n = pick([name[1] for name in pairs], step), pick([name[2] for name in pairs], step)
        a, b = xs(pick([OFF[name[1]] for name in pairs], step)), xs(pick([OFF[name[2]] for name in pairs], step))
        scale = HEAD**-0.5 * LOG2E
        base, keys = bias[a], bias[b]
        cuts = [(i * TOK, -(-(i + 1) * TOK // HEAD) * HEAD) for i in range(NY)]
        rows = [pl.ds(first, TOK) for first, _ in cuts]
        old = [(high[m, at], total[m, at], summed[m, at]) for at in rows]
        scores = [lax.dot_general(qkv[m, at, :HEAD], qkv[n, :width, HEAD : 2 * HEAD], (((1,), (1,)), ((), ())),
                                  preferred_element_type=jnp.float32) for at, (_, width) in zip(rows, cuts)]
        reach = jnp.clip(lax.broadcasted_iota(jnp.int32, (TOK, HEAD), 0) + (a - b) * TOK, -1, TOK - 1)
        lane = lax.broadcasted_iota(jnp.int32, (TOK, HEAD), 1)
        parts, tops = [], []
        for one, (first, width) in zip(scores, cuts):
            at = -(-first // HEAD) * HEAD
            shift = base[:, at : at + 1] - keys[:, :width]
            some = []
            for at in range(0, width, HEAD):
                part_of = one[:, at : at + HEAD] * scale + shift[:, at : at + HEAD]
                if at + HEAD > first:
                    part_of = jnp.where(lane + (at - first) <= reach, part_of, -1e30)
                some.append(part_of)
            parts.append(some)
            tops.append(jnp.max(fold(some, jnp.maximum), axis=1, keepdims=True))
        new = []
        for some, most, (before_, _, _), (_, width) in zip(parts, tops, old, cuts):
            top = jnp.maximum(before_, most)
            less = jnp.exp2(before_ - top)
            some = [jnp.exp2(one - top) for one in some]
            rounded = jnp.concatenate([one.astype(jnp.bfloat16) for one in some], axis=1)
            value = jnp.dot(rounded, qkv[n, :width, 2 * HEAD :], preferred_element_type=jnp.float32)
            new.append((top, less, fold(some, jnp.add), value))
        for at, (top, less, low, value), (_, total_, summed_) in zip(rows, new, old):
            high[m, at] = top
            total[m, at] = total_ * less + low
            summed[m, at] = summed_ * less + value

    def finish(m):
        heads[m] = (summed[m] / jnp.sum(total[m], axis=1, keepdims=True)).astype(jnp.bfloat16)
        for r in (2, 1, 3, 0):
            if m or r:
                start(("O", m, r, 0))
            else:
                local.start()

    last = {name[1]: name for name in pairs}
    loop(pairs, pair, {name: functools.partial(finish, m) for m, name in last.items()})
    for m in range(NX):
        for r in range(NY):
            if m or r:
                arrival(("O", m, r, 0))
    local.wait()
    for name in started:
        source, target, _, who = regions(name)
        copy_of(name, source, target, who).wait_send()


def merge(heads, out, held, sem):
    come = [pltpu.make_async_copy(heads.at[i], held.at[i], sem.at[0, i]) for i in range(NX * NY)]
    go = [pltpu.make_async_copy(held.at[i], out.at[:, pl.ds(i * HEAD, HEAD)], sem.at[1, i]) for i in range(NX * NY)]
    for copy in come:
        copy.start()
    for one, other in zip(come, go):
        one.wait()
        other.start()
    for copy in go:
        copy.wait()


def body(tokens, query_weight, key_weight, value_weight, cum_gate):
    count = sum(len(m) for m in (weight_messages(), token_messages(), *map(exchange_messages, range(NX))))
    any_space = pl.BlockSpec(memory_space=pl.ANY)
    vmem_space = pl.BlockSpec(memory_space=pltpu.VMEM)
    attended = pl.pallas_call(
        kernel,
        out_shape=jax.ShapeDtypeStruct((NX * NY, TOK, HEAD), jnp.bfloat16),
        in_specs=[any_space] * 4 + [vmem_space],
        out_specs=any_space,
        scratch_shapes=[
            pltpu.VMEM((D, NY * 3 * HEAD), jnp.bfloat16),
            pltpu.VMEM((NX, TOK, D), jnp.bfloat16),
            pltpu.VMEM((NX, TOK, NY * QKV), jnp.bfloat16),
            pltpu.VMEM((NX, 2, HALF, QKV), jnp.bfloat16),
            pltpu.VMEM((NX, GROUP, QKV), jnp.bfloat16),
            pltpu.VMEM((NX, 1, GROUP), jnp.float32),
            pltpu.VMEM((NX, GROUP, HEAD), jnp.float32),
            pltpu.VMEM((NX, GROUP, HEAD), jnp.float32),
            pltpu.VMEM((NX, GROUP, HEAD), jnp.float32),
            pltpu.VMEM((NX, GROUP, HEAD), jnp.bfloat16),
            pltpu.SemaphoreType.DMA((5,)),
            pltpu.SemaphoreType.DMA((count + NX * NY,)),
            pltpu.SemaphoreType.DMA((count + NX * NY,)),
        ],
        compiler_params=pltpu.CompilerParams(
            collective_id=0, has_side_effects=True, vmem_limit_bytes=60 * 1024 * 1024
        ),
        name="mixer",
    )(tokens[0], query_weight, key_weight, value_weight, cum_gate[0])
    merged = pl.pallas_call(
        merge,
        out_shape=jax.ShapeDtypeStruct((TOK, NX * NY * HEAD), jnp.bfloat16),
        in_specs=[any_space],
        out_specs=any_space,
        scratch_shapes=[pltpu.VMEM((NX * NY, TOK, HEAD), jnp.bfloat16), pltpu.SemaphoreType.DMA((2, NX * NY))],
        name="merge",
    )(attended)
    return merged[None]


def solution(mesh):
    in_specs = (
        P("dp", "sp", None),
        P("dp", "sp"),
        P("dp", "sp"),
        P("dp", "sp"),
        P("dp", "sp", None),
    )
    out_specs = P("dp", "sp", None)
    return jax.shard_map(body, mesh=mesh, in_specs=in_specs, out_specs=out_specs, check_vma=False)
```

```python
import functools

import jax
import jax.numpy as jnp
from jax import lax
from jax.experimental import pallas as pl
from jax.experimental.pallas import tpu as pltpu
from jax.sharding import PartitionSpec as P

MESH = pl.DeviceIdType.MESH
NX, NY, NZ = 4, 4, 8
TOK, D, HEAD = 192, 4096, 128
HALF = TOK // 2
ROWS = 256
LEN = 3072
GROUP = NY * TOK
LOG2E = 1.4426950408889634

QKV = 3 * HEAD
A_ROWS = 96
ORDER = (0, -1, 1, -2, 2, -3, 3, 4)
OFF = (0, -1, 1, 2)
BATCHES = ((0,), (1, 2), (3,))
TILE_US, PAIR_US = (0.65, 1.05, 0.65), 1.75
PAIRS = (((0, 0), (1, 1)), ((0, 1), (1, 0)), ((2, 2), (1, 2)), ((2, 0), (2, 1)),
         ((3, 3), (1, 3)), ((3, 0), (2, 3)), ((3, 1), (3, 2)), ((0, 2), (0, 3)))
DONE = {4: (1,), 5: (2,), 6: (3,), 7: (0,)}
SPLIT = tuple((m, r) for m in (3, 1, 2, 0) for r in range(NY) if m == 3 or r == 2)
TILES = (3, 4, 5, 2, 1, 0)


def weight_messages():
    a, b, g = A_ROWS * QKV * 2, (ROWS - A_ROWS) * QKV * 2, 0
    m = {}
    for sign, link in ((1, "y+"), (-1, "y-")):
        m["Ay", g, sign, 0] = (link, a, [])
    for sign, link in ((1, "y+"), (-1, "y-")):
        m["Af", g, sign, 0] = (link, a / 2, [("Ay", g, sign, 0)])
    first = [(kind, g, sign, 0) for kind in ("Ay", "Af") for sign in (1, -1)]

    def along_z(kind, size, need):
        for sign, link in ((1, "z+"), (-1, "z-")):
            for t in range(1, 5):
                m[kind, g, sign, t] = (link, size * (0.5 if t == 4 else 1), [(kind, g, sign, t - 1)] if t > 1 else need)

    def block(kind, off, own):
        if off == 0:
            return own
        if off == 4:
            return [(kind, g, 1, 4), (kind, g, -1, 4)]
        return [(kind, g, 1 if off < 0 else -1, abs(off))]

    if b:
        along_z("Bz", b, [])
        for off in ORDER:
            need = block("Bz", off, [])
            for sign, link in ((1, "y+"), (-1, "y-")):
                m["By", g, sign, off] = (link, b, need)
                m["Bf", g, sign, off] = (link, b / 2, [("By", g, sign, off)])
            m["Bd", g, 0, off] = ("d", b * 4, [(kind, g, sign, off) for kind in ("By", "Bf") for sign in (1, -1)])
    along_z("Az", a * 4, first)
    for off in ORDER:
        m["Ad", g, 0, off] = ("d", a * 4, block("Az", off, first))
    return m


def token_messages():
    h = HALF * D * 2
    m = {}
    for i in range(3):
        for sign, link in ((1, "x+"), (-1, "x-")):
            m["T", 0, sign, i] = (link, h, [("T", 0, sign, 0)] if i == 2 else [])
    return m


def batch_of(n):
    return next(i for i, batch in enumerate(BATCHES) if n in batch)


def exchange_messages(n):
    m = {}
    size = TOK * QKV * 2
    for sign, link in ((1, "y+"), (-1, "y-")):
        m["Er", 0, sign, n] = (link, size / 2, [("tile", batch_of(n), 3), ("tile", batch_of(n), 4)])
        m["Ef", 0, sign, n] = (link, size / 2, [("Er", 0, sign, n)])
        m["Ey", 0, sign, n] = (link, size, [("tile", batch_of(n), 5 if sign < 0 else 1)])
    return m


def tasks():
    t = {}
    tokens = ([], [("T", 0, 1, 0), ("T", 0, 1, 1)], [("T", 0, -1, 0), ("T", 0, -1, 1)], [("T", 0, 1, 2), ("T", 0, -1, 2)])
    for i, batch in enumerate(BATCHES):
        for j in TILES:
            need = [k for n in batch for k in tokens[n]] + list(weight_messages())
            t["tile", i, j] = (TILE_US[i], need)
    done = [[(kind, 0, sign, n) for kind in ("Ey", "Ef") for sign in (1, -1)] for n in range(NX)]
    for k, some in enumerate(PAIRS):
        t["pair", k, 0] = (PAIR_US, [one for mn in some for i in mn for one in done[i]])
    names = list(t)
    for before, name in zip(names, names[1:]):
        t[name][1].append(before)
    return t


def schedule():
    messages = {}
    for some in (weight_messages(), token_messages(), *(exchange_messages(n) for n in range(NX))):
        messages.update(some)
    work = tasks()
    place = {name: i for i, name in enumerate([*messages, *work])}
    done, free, order, now = {}, {}, [], 0.0
    left = dict.fromkeys(place)
    while left:
        ready = []
        for name in left:
            need = messages[name][2] if name in messages else work[name][1]
            if all(k in done for k in need):
                at = max([done[k] for k in need], default=0.0)
                ready.append((max(at, now), name in work, at if name in messages else 0.0, place[name], name))
        at, heavy, _, _, name = min(ready)
        del left[name]
        order.append(name)
        now = at
        if heavy:
            now += work[name][0]
            done[name] = now
        else:
            link, size, _ = messages[name]
            end = max(now, free.get(link, 0.0)) + (size / 600e3 if link == "d" else size / 45e3)
            free[link] = end
            done[name] = end + (1.0 if link == "d" else 1.8)
    return order, messages, work, done, free


def mo(v, n):
    return pl.multiple_of(v, n)


def fold(parts, op):
    return functools.reduce(op, parts)


def kernel(tok, wq, wk, wv, gate, out, w, t, p, relay, qkv, bias, high, total, summed, heads, relay_out,
           load_sem, send_sem, recv_sem):
    s, d = lax.axis_index("sp"), lax.axis_index("dp")
    y, x = lax.div(s, NX), lax.rem(s, NX)
    z, c = lax.div(d, 2), lax.rem(d, 2)

    def xs(i):
        return lax.rem(x + NX + i, NX)

    def ys(i):
        return lax.rem(y + NY + i, NY)

    def zs(i):
        return lax.rem(z + NZ + i, NZ)

    def dev(dx=0, dy=0, dz=0, other=False):
        return {"sp": ys(dy) * NX + xs(dx), "dp": zs(dz) * 2 + (1 - c if other else c)}

    own = pl.ds(mo(d * ROWS, ROWS), ROWS)
    loads = []
    for i, (ref, at) in enumerate(((wq, 0), (wk, HEAD), (wv, 2 * HEAD))):
        loads.append(pltpu.make_async_copy(ref, w.at[own, pl.ds(at, HEAD)], load_sem.at[i]))
    loads.append(pltpu.make_async_copy(tok, t.at[0], load_sem.at[3]))
    for copy in loads:
        copy.start()

    barrier = pltpu.get_barrier_semaphore()
    greet = [dev(dx=dx, dy=dy) for dy in range(NY) for dx in range(NX) if dx or dy]
    greet += [dev(dz=1), dev(dz=-1), dev(other=True)]
    for who in greet:
        pl.semaphore_signal(barrier, inc=1, device_id=who, device_id_type=MESH)
    for b in range(NX):
        bias[b] = LOG2E * jnp.concatenate(
            [gate[0:1, (NX * i + b) * TOK : (NX * i + b + 1) * TOK] for i in range(NY)], axis=1)
    pl.semaphore_wait(barrier, len(greet))

    def wrect(zo, row0, rows, col=None, other=False):
        core = 1 - c if other else c
        at = pl.ds(mo((zs(zo) * 2 + core) * ROWS + row0, 16), rows)
        if col is None:
            return w.at[at]
        return w.at[at, pl.ds(col % NY * QKV, QKV)]

    def part(sign):
        return 0 if sign == 1 else HALF

    def seat(n, dy, at=0, count=TOK):
        return qkv.at[n, pl.ds(mo(ys(dy) * TOK + at, 16), count)]

    def regions(name):
        kind, g, sign, i = name
        if kind == "T":
            near = OFF.index(-sign)
            if i == 2:
                at = pl.ds(part(sign), HALF)
                return t.at[near, at], t.at[3, at], t.at[3, at], dev(dx=sign)
            at = pl.ds(part(sign) if i == 0 else part(-sign), HALF)
            return t.at[0, at], t.at[near, at], t.at[near, at], dev(dx=sign)
        if kind == "O":
            count = HALF if (g, sign) in SPLIT else TOK
            source = heads.at[g, pl.ds(mo(ys(sign) * TOK, 16), count)]
            rows = pl.ds(0, count)
            return source, out.at[s, rows], out.at[ys(-sign) * NX + xs(-OFF[g]), rows], dev(dx=OFF[g], dy=sign)
        if kind in ("R", "F"):
            hop = relay_out.at[SPLIT.index((g, sign))]
            near = (-1 if g == 3 else OFF[g], -1 if sign == 2 else sign)
            if kind == "R":
                return heads.at[g, pl.ds(mo(ys(sign) * TOK + HALF, 16), HALF)], hop, hop, dev(*near)
            rows = pl.ds(HALF, HALF)
            return (hop, out.at[ys(-near[1]) * NX + xs(-near[0]), rows],
                    out.at[ys(-sign) * NX + xs(-OFF[g]), rows], dev(-1 if g == 3 else 0, -1 if sign == 2 else 0))
        if kind[0] == "E":
            hop = relay.at[i, 0 if sign == 1 else 1]

            def stage(r, at=0, count=TOK):
                return p.at[i, pl.ds(at, count), pl.ds(r * QKV, QKV)]

            if kind == "Er":
                return stage(2, part(sign), HALF), hop, hop, dev(dy=sign)
            if kind == "Ef":
                return (hop, seat(i, -sign, part(sign), HALF), seat(i, -2 * sign, part(sign), HALF),
                        dev(dy=sign))
            return stage(sign % NY), seat(i, 0), seat(i, -sign), dev(dy=sign)
        row0, rows = (0, A_ROWS) if kind[0] == "A" else (A_ROWS, ROWS - A_ROWS)
        half = rows // 2
        if kind[1] == "z":
            col = None if kind == "Az" else 0
            if i == 4:
                row0, rows = row0 + (0 if sign == 1 else half), half
            source = wrect(-sign * (i - 1), row0, rows, col)
            return source, source, wrect(-sign * i, row0, rows, col), dev(dz=sign)
        if kind[1] == "y":
            return wrect(i, row0, rows, 0), wrect(i, row0, rows, -sign), wrect(i, row0, rows, -sign), dev(dy=sign)
        if kind[1] == "f":
            row0, rows = row0 + (0 if sign == 1 else half), half
            return wrect(i, row0, rows, -sign), wrect(i, row0, rows, 2), wrect(i, row0, rows, 2), dev(dy=sign)
        source = wrect(i, row0, rows)
        return source, source, wrect(i, row0, rows, other=True), dev(other=True)

    started, arrived, number = [], set(), {}

    def copy_of(name, source, target, who):
        n = number.setdefault(name, len(number))
        return pltpu.make_async_remote_copy(
            src_ref=source, dst_ref=target, send_sem=send_sem.at[n], recv_sem=recv_sem.at[n],
            device_id=who, device_id_type=MESH)

    def start(name):
        source, target, _, who = regions(name)
        copy_of(name, source, target, who).start()
        started.append(name)

    def arrival(name):
        if name not in arrived:
            arrived.add(name)
            _, _, where, who = regions(name)
            copy_of(name, where, where, who).wait_recv()

    order, messages, work, _, _ = schedule()
    loaded = set()

    def message(name):
        for i in (3,) if name[0] == "T" else (0, 1, 2) if name[0][0] in "AB" else ():
            if i not in loaded:
                loaded.add(i)
                loads[i].wait()
        for need in messages[name][2]:
            if need in messages:
                arrival(need)
        start(name)

    names = [name for name in order if name in work]
    ahead = {}
    waiting = []
    for name in order:
        if name in work:
            ahead[name] = waiting
            waiting = []
        else:
            waiting.append(name)

    def before(name):
        previous = names.index(name) - 1
        if previous >= 0:
            kind, i, j = names[previous]
            if kind == "tile" and j == TILES[-1]:
                for n in BATCHES[i]:
                    qkv[n, pl.ds(mo(y * TOK, TOK), TOK)] = p[n, :, :QKV]
        for item in ahead[name]:
            message(item)
        if name == names[-1]:
            for m, r in SPLIT:
                if m in (1, 2):
                    arrival(("R", m, r, 0))
                    start(("F", m, r, 0))
        for need in work[name][1]:
            if need in messages:
                arrival(need)

    def loop(some, run, after=None):
        before(some[0])

        @pl.loop(0, len(some))
        def _(step):
            for k, name in enumerate(some):
                if k:
                    @pl.when(step == k)
                    def _():
                        before(name)
            run(step)
            for k, name in enumerate(some):
                if after and name in after:
                    @pl.when(step == k)
                    def _():
                        after[name]()

    def pick(values, step):
        value = jnp.int32(values[0])
        for k in range(1, len(values)):
            if values[k] != values[k - 1]:
                value = jnp.where(step >= k, values[k], value)
        return value

    for i, batch in enumerate(BATCHES):
        def tile(step):
            j = pick(TILES, step)
            rows = t[batch[0] : batch[-1] + 1].reshape(len(batch) * TOK, D)
            rows = jnp.dot(rows, w[:, pl.ds(mo(j * 256, 256), 256)], preferred_element_type=jnp.float32)
            rows = rows.astype(jnp.bfloat16).reshape(len(batch), TOK, 256)
            for n, block in zip(batch, rows):
                p[n, :, pl.ds(mo(j * 256, 256), 256)] = block

        loop([("tile", i, j) for j in TILES], tile)

    pairs = [name for name in names if name[0] == "pair"]
    local = pltpu.make_async_copy(heads.at[0, pl.ds(mo(y * TOK, 16), TOK)], out.at[s], load_sem.at[4])

    for m in range(NX):
        high[m] = jnp.full((GROUP, HEAD), -1e30, jnp.float32)
        total[m] = jnp.zeros((GROUP, HEAD), jnp.float32)
        summed[m] = jnp.zeros((GROUP, HEAD), jnp.float32)

    def pair(step, which):
        m, n = (pick([some[which][i] for some in PAIRS], step) for i in (0, 1))
        a, b = (xs(pick([OFF[some[which][i]] for some in PAIRS], step)) for i in (0, 1))
        scale = HEAD**-0.5 * LOG2E
        base, keys = bias[a], bias[b]
        cuts = [(i * TOK, -(-(i + 1) * TOK // HEAD) * HEAD) for i in range(NY)]
        rows = [pl.ds(first, TOK) for first, _ in cuts]
        old = [(high[m, at], total[m, at], summed[m, at]) for at in rows]
        scores = [lax.dot_general(qkv[m, at, :HEAD], qkv[n, :width, HEAD : 2 * HEAD], (((1,), (1,)), ((), ())),
                                  preferred_element_type=jnp.float32) for at, (_, width) in zip(rows, cuts)]
        reach = jnp.clip(lax.broadcasted_iota(jnp.int32, (TOK, HEAD), 0) + (a - b) * TOK, -1, TOK - 1)
        lane = lax.broadcasted_iota(jnp.int32, (TOK, HEAD), 1)
        parts, tops = [], []
        for one, (first, width) in zip(scores, cuts):
            at = -(-first // HEAD) * HEAD
            shift = base[:, at : at + 1] - keys[:, :width]
            some = []
            for at in range(0, width, HEAD):
                part_of = one[:, at : at + HEAD] * scale + shift[:, at : at + HEAD]
                if at + HEAD > first:
                    part_of = jnp.where(lane + (at - first) <= reach, part_of, -1e30)
                some.append(part_of)
            parts.append(some)
            tops.append(jnp.max(fold(some, jnp.maximum), axis=1, keepdims=True))
        new = []
        for some, most, (before_, _, _), (_, width) in zip(parts, tops, old, cuts):
            top = jnp.maximum(before_, most)
            less = jnp.exp2(before_ - top)
            some = [jnp.exp2(one - top) for one in some]
            rounded = jnp.concatenate([one.astype(jnp.bfloat16) for one in some], axis=1)
            value = jnp.dot(rounded, qkv[n, :width, 2 * HEAD :], preferred_element_type=jnp.float32)
            new.append((top, less, fold(some, jnp.add), value))
        for at, (top, less, low, value), (_, total_, summed_) in zip(rows, new, old):
            high[m, at] = top
            total[m, at] = total_ * less + low
            summed[m, at] = summed_ * less + value

    def finish(m):
        heads[m] = (summed[m] / jnp.sum(total[m], axis=1, keepdims=True)).astype(jnp.bfloat16)
        for r in (2, 1, 3, 0):
            if (m, r) in SPLIT:
                start(("R", m, r, 0))
        for r in (2, 1, 3, 0):
            if m or r:
                start(("O", m, r, 0))
            else:
                local.start()

    def run(step):
        pair(step, 0)
        pair(step, 1)

    loop(pairs, run, {pairs[k]: functools.partial(lambda ms: [finish(m) for m in ms], ms) for k, ms in DONE.items()})
    for m, r in SPLIT:
        if m in (0, 3):
            arrival(("R", m, r, 0))
            start(("F", m, r, 0))
    for m in range(NX):
        for r in range(NY):
            if m or r:
                arrival(("O", m, r, 0))
    for m, r in SPLIT:
        arrival(("F", m, r, 0))
    local.wait()
    for name in started:
        source, target, _, who = regions(name)
        copy_of(name, source, target, who).wait_send()


def merge(heads, out, held, sem):
    come = [pltpu.make_async_copy(heads.at[i], held.at[i], sem.at[0, i]) for i in range(NX * NY)]
    go = [pltpu.make_async_copy(held.at[i], out.at[:, pl.ds(i * HEAD, HEAD)], sem.at[1, i]) for i in range(NX * NY)]
    for copy in come:
        copy.start()
    for one, other in zip(come, go):
        one.wait()
        other.start()
    for copy in go:
        copy.wait()


def body(tokens, query_weight, key_weight, value_weight, cum_gate):
    count = sum(len(m) for m in (weight_messages(), token_messages(), *map(exchange_messages, range(NX))))
    any_space = pl.BlockSpec(memory_space=pl.ANY)
    vmem_space = pl.BlockSpec(memory_space=pltpu.VMEM)
    attended = pl.pallas_call(
        kernel,
        out_shape=jax.ShapeDtypeStruct((NX * NY, TOK, HEAD), jnp.bfloat16),
        in_specs=[any_space] * 4 + [vmem_space],
        out_specs=any_space,
        scratch_shapes=[
            pltpu.VMEM((D, NY * 3 * HEAD), jnp.bfloat16),
            pltpu.VMEM((NX, TOK, D), jnp.bfloat16),
            pltpu.VMEM((NX, TOK, NY * QKV), jnp.bfloat16),
            pltpu.VMEM((NX, 2, HALF, QKV), jnp.bfloat16),
            pltpu.VMEM((NX, GROUP, QKV), jnp.bfloat16),
            pltpu.VMEM((NX, 1, GROUP), jnp.float32),
            pltpu.VMEM((NX, GROUP, HEAD), jnp.float32),
            pltpu.VMEM((NX, GROUP, HEAD), jnp.float32),
            pltpu.VMEM((NX, GROUP, HEAD), jnp.float32),
            pltpu.VMEM((NX, GROUP, HEAD), jnp.bfloat16),
            pltpu.VMEM((len(SPLIT), HALF, HEAD), jnp.bfloat16),
            pltpu.SemaphoreType.DMA((5,)),
            pltpu.SemaphoreType.DMA((count + NX * NY + 2 * len(SPLIT),)),
            pltpu.SemaphoreType.DMA((count + NX * NY + 2 * len(SPLIT),)),
        ],
        compiler_params=pltpu.CompilerParams(
            collective_id=0, has_side_effects=True, vmem_limit_bytes=60 * 1024 * 1024
        ),
        name="mixer",
    )(tokens[0], query_weight, key_weight, value_weight, cum_gate[0])
    merged = pl.pallas_call(
        merge,
        out_shape=jax.ShapeDtypeStruct((TOK, NX * NY * HEAD), jnp.bfloat16),
        in_specs=[any_space],
        out_specs=any_space,
        scratch_shapes=[pltpu.VMEM((NX * NY, TOK, HEAD), jnp.bfloat16), pltpu.SemaphoreType.DMA((2, NX * NY))],
        name="merge",
    )(attended)
    return merged[None]


def solution(mesh):
    in_specs = (
        P("dp", "sp", None),
        P("dp", "sp"),
        P("dp", "sp"),
        P("dp", "sp"),
        P("dp", "sp", None),
    )
    out_specs = P("dp", "sp", None)
    return jax.shard_map(body, mesh=mesh, in_specs=in_specs, out_specs=out_specs, check_vma=False)
```

```python
import functools

import jax
import jax.numpy as jnp
from jax import lax
from jax.experimental import pallas as pl
from jax.experimental.pallas import tpu as pltpu
from jax.sharding import PartitionSpec as P

MESH = pl.DeviceIdType.MESH
NX, NY, NZ = 4, 4, 8
TOK, D, HEAD = 192, 4096, 128
HALF = TOK // 2
ROWS = 256
LEN = 3072
GROUP = NY * TOK
LOG2E = 1.4426950408889634

WIDE = (2 * HEAD, HEAD)
FIRST = (0, NY * 2 * HEAD)
QKV = 3 * HEAD
A_ROWS = (64, 224)
ORDER = (0, -1, 1, -2, 2, -3, 3, 4)
OFF = (0, -1, 1, 2)
LOOPS = (((0,), (2, 3, 1, 0), 0.65), ((1, 2), (2, 3, 1, 0), 1.05), ((0, 1, 2), (5, 4), 1.4), ((3,), (2, 3, 1, 0, 5, 4), 0.65))
PAIR_US = 1.75
RELAY_US = 4.0
PAIRS = (((0, 0), (1, 1)), ((0, 1), (1, 0)), ((2, 2), (1, 2)), ((2, 0), (2, 1)),
         ((3, 3), (1, 3)), ((3, 0), (2, 3)), ((3, 1), (3, 2)), ((0, 2), (0, 3)))
DONE = {4: (1,), 5: (2,), 6: (3,), 7: (0,)}
SPLIT = tuple((m, r) for m in (3, 1, 2, 0) for r in range(NY) if m == 3 or r == 2)
TILES = (3, 4, 5, 2, 1, 0)


def weight_messages(g):
    a, b = A_ROWS[g] * WIDE[g] * 2, (ROWS - A_ROWS[g]) * WIDE[g] * 2
    m = {}
    for sign, link in ((1, "y+"), (-1, "y-")):
        m["Ay", g, sign, 0] = (link, a, [])
    for sign, link in ((1, "y+"), (-1, "y-")):
        m["Af", g, sign, 0] = (link, a / 2, [("Ay", g, sign, 0)])
    first = [(kind, g, sign, 0) for kind in ("Ay", "Af") for sign in (1, -1)]

    def along_z(kind, size, need):
        for sign, link in ((1, "z+"), (-1, "z-")):
            for t in range(1, 5):
                m[kind, g, sign, t] = (link, size * (0.5 if t == 4 else 1), [(kind, g, sign, t - 1)] if t > 1 else need)

    def block(kind, off, own):
        if off == 0:
            return own
        if off == 4:
            return [(kind, g, 1, 4), (kind, g, -1, 4)]
        return [(kind, g, 1 if off < 0 else -1, abs(off))]

    if b:
        along_z("Bz", b, [])
        for off in ORDER:
            need = block("Bz", off, [])
            for sign, link in ((1, "y+"), (-1, "y-")):
                m["By", g, sign, off] = (link, b, need)
                m["Bf", g, sign, off] = (link, b / 2, [("By", g, sign, off)])
            m["Bd", g, 0, off] = ("d", b * 4, [(kind, g, sign, off) for kind in ("By", "Bf") for sign in (1, -1)])
    along_z("Az", a * 4, first)
    for off in ORDER:
        m["Ad", g, 0, off] = ("d", a * 4, block("Az", off, first))
    return m


def token_messages():
    h = HALF * D * 2
    m = {}
    for i in range(3):
        for sign, link in ((1, "x+"), (-1, "x-")):
            m["T", 0, sign, i] = (link, h, [("T", 0, sign, 0)] if i == 2 else [])
    return m


def tile_of(n, j):
    return next(("tile", i, j) for i, (blocks, tiles, _) in enumerate(LOOPS) if n in blocks and j in tiles)


def exchange_messages(n):
    m = {}
    for g in (0, 1):
        size = TOK * WIDE[g] * 2
        tile = [tile_of(n, r if g == 0 else 4 + r // 2) for r in range(NY)]
        for sign, link in ((1, "y+"), (-1, "y-")):
            m["Er", g, sign, n] = (link, size / 2, [tile[2]])
            m["Ef", g, sign, n] = (link, size / 2, [("Er", g, sign, n)])
            m["Ey", g, sign, n] = (link, size, [tile[sign % NY]])
    return m


def tasks():
    t = {}
    tokens = ([], [("T", 0, 1, 0), ("T", 0, 1, 1)], [("T", 0, -1, 0), ("T", 0, -1, 1)], [("T", 0, 1, 2), ("T", 0, -1, 2)])
    for i, (blocks, tiles, time) in enumerate(LOOPS):
        for j in tiles:
            t["tile", i, j] = (time, [k for n in blocks for k in tokens[n]] + list(weight_messages(j // 4)))
    done = [[[(kind, g, sign, n) for kind in ("Ey", "Ef") for sign in (1, -1)] for n in range(NX)] for g in (0, 1)]
    for k, some in enumerate(PAIRS):
        t["pair", k, 0] = (PAIR_US, [one for q, k_ in some for one in done[1][q] + done[0][k_]])
    names = list(t)
    for before, name in zip(names, names[1:]):
        t[name][1].append(before)
    return t


def schedule():
    messages = {}
    for some in (weight_messages(0), token_messages(), weight_messages(1), *(exchange_messages(n) for n in range(NX))):
        messages.update(some)
    work = tasks()
    place = {name: i for i, name in enumerate([*messages, *work])}
    done, free, order, now = {}, {}, [], 0.0
    left = dict.fromkeys(place)
    while left:
        ready = []
        for name in left:
            need = messages[name][2] if name in messages else work[name][1]
            if all(k in done for k in need):
                at = max([done[k] for k in need], default=0.0)
                ready.append((max(at, now), name in work, at if name in messages else 0.0, place[name], name))
        at, heavy, _, _, name = min(ready)
        del left[name]
        order.append(name)
        now = at
        if heavy:
            now += work[name][0]
            done[name] = now
        else:
            link, size, _ = messages[name]
            end = max(now, free.get(link, 0.0)) + (size / 600e3 if link == "d" else size / 45e3)
            free[link] = end
            done[name] = end + (1.0 if link == "d" else RELAY_US if name[0] == "Er" and name[3] < 3 else 1.8)
    return order, messages, work, done, free


def mo(v, n):
    return pl.multiple_of(v, n)


def fold(parts, op):
    return functools.reduce(op, parts)


def kernel(tok, wq, wk, wv, gate, out, w, t, p, relay_kv, relay_q, kv, qs, bias, high, total, summed, heads, relay_out,
           load_sem, send_sem, recv_sem):
    s, d = lax.axis_index("sp"), lax.axis_index("dp")
    y, x = lax.div(s, NX), lax.rem(s, NX)
    z, c = lax.div(d, 2), lax.rem(d, 2)

    def xs(i):
        return lax.rem(x + NX + i, NX)

    def ys(i):
        return lax.rem(y + NY + i, NY)

    def zs(i):
        return lax.rem(z + NZ + i, NZ)

    def dev(dx=0, dy=0, dz=0, other=False):
        return {"sp": ys(dy) * NX + xs(dx), "dp": zs(dz) * 2 + (1 - c if other else c)}

    own = pl.ds(mo(d * ROWS, ROWS), ROWS)
    loads = []
    for i, (ref, at) in enumerate(((wk, 0), (wv, HEAD), (wq, FIRST[1]))):
        loads.append(pltpu.make_async_copy(ref, w.at[own, pl.ds(at, HEAD)], load_sem.at[i]))
    loads.append(pltpu.make_async_copy(tok, t.at[0], load_sem.at[3]))
    for copy in loads:
        copy.start()

    barrier = pltpu.get_barrier_semaphore()
    greet = [dev(dx=dx, dy=dy) for dy in range(NY) for dx in range(NX) if dx or dy]
    greet += [dev(dz=1), dev(dz=-1), dev(other=True)]
    for who in greet:
        pl.semaphore_signal(barrier, inc=1, device_id=who, device_id_type=MESH)
    for b in range(NX):
        bias[b] = LOG2E * jnp.concatenate(
            [gate[0:1, (NX * i + b) * TOK : (NX * i + b + 1) * TOK] for i in range(NY)], axis=1)
    pl.semaphore_wait(barrier, len(greet))

    def wrect(g, zo, row0, rows, col=None, other=False):
        core = 1 - c if other else c
        at = pl.ds(mo((zs(zo) * 2 + core) * ROWS + row0, 16), rows)
        if col is None:
            return w.at[at, pl.ds(FIRST[g], NY * WIDE[g])]
        return w.at[at, pl.ds(FIRST[g] + col % NY * WIDE[g], WIDE[g])]

    def part(sign):
        return 0 if sign == 1 else HALF

    def seat(g, n, dy, at=0, count=TOK):
        return (kv, qs)[g].at[n, pl.ds(mo(ys(dy) * TOK + at, 16), count)]

    def regions(name):
        kind, g, sign, i = name
        if kind == "T":
            near = OFF.index(-sign)
            if i == 2:
                at = pl.ds(part(sign), HALF)
                return t.at[near, at], t.at[3, at], t.at[3, at], dev(dx=sign)
            at = pl.ds(part(sign) if i == 0 else part(-sign), HALF)
            return t.at[0, at], t.at[near, at], t.at[near, at], dev(dx=sign)
        if kind == "O":
            count = HALF if (g, sign) in SPLIT else TOK
            source = heads.at[g, pl.ds(mo(ys(sign) * TOK, 16), count)]
            rows = pl.ds(0, count)
            return source, out.at[s, rows], out.at[ys(-sign) * NX + xs(-OFF[g]), rows], dev(dx=OFF[g], dy=sign)
        if kind in ("R", "F"):
            hop = relay_out.at[SPLIT.index((g, sign))]
            near = (-1 if g == 3 else OFF[g], -1 if sign == 2 else sign)
            if kind == "R":
                return heads.at[g, pl.ds(mo(ys(sign) * TOK + HALF, 16), HALF)], hop, hop, dev(*near)
            rows = pl.ds(HALF, HALF)
            return (hop, out.at[ys(-near[1]) * NX + xs(-near[0]), rows],
                    out.at[ys(-sign) * NX + xs(-OFF[g]), rows], dev(-1 if g == 3 else 0, -1 if sign == 2 else 0))
        if kind[0] == "E":
            hop = (relay_kv, relay_q)[g].at[i, 0 if sign == 1 else 1]

            def stage(r, at=0, count=TOK):
                if g == 0:
                    return p.at[i, r, pl.ds(at, count)]
                return p.at[i, 4 + r // 2, pl.ds(at, count), pl.ds(r % 2 * HEAD, HEAD)]

            if kind == "Er":
                return stage(2, part(sign), HALF), hop, hop, dev(dy=sign)
            if kind == "Ef":
                return (hop, seat(g, i, -sign, part(sign), HALF), seat(g, i, -2 * sign, part(sign), HALF),
                        dev(dy=sign))
            return stage(sign % NY), seat(g, i, 0), seat(g, i, -sign), dev(dy=sign)
        row0, rows = (0, A_ROWS[g]) if kind[0] == "A" else (A_ROWS[g], ROWS - A_ROWS[g])
        half = rows // 2
        if kind[1] == "z":
            col = None if kind == "Az" else 0
            if i == 4:
                row0, rows = row0 + (0 if sign == 1 else half), half
            source = wrect(g, -sign * (i - 1), row0, rows, col)
            return source, source, wrect(g, -sign * i, row0, rows, col), dev(dz=sign)
        if kind[1] == "y":
            return wrect(g, i, row0, rows, 0), wrect(g, i, row0, rows, -sign), wrect(g, i, row0, rows, -sign), dev(dy=sign)
        if kind[1] == "f":
            row0, rows = row0 + (0 if sign == 1 else half), half
            return wrect(g, i, row0, rows, -sign), wrect(g, i, row0, rows, 2), wrect(g, i, row0, rows, 2), dev(dy=sign)
        source = wrect(g, i, row0, rows)
        return source, source, wrect(g, i, row0, rows, other=True), dev(other=True)

    started, arrived, number = [], set(), {}

    def copy_of(name, source, target, who):
        n = number.setdefault(name, len(number))
        return pltpu.make_async_remote_copy(
            src_ref=source, dst_ref=target, send_sem=send_sem.at[n], recv_sem=recv_sem.at[n],
            device_id=who, device_id_type=MESH)

    def start(name):
        source, target, _, who = regions(name)
        copy_of(name, source, target, who).start()
        started.append(name)

    def arrival(name):
        if name not in arrived:
            arrived.add(name)
            _, _, where, who = regions(name)
            copy_of(name, where, where, who).wait_recv()

    order, messages, work, _, _ = schedule()
    loaded = set()

    def message(name):
        for i in (3,) if name[0] == "T" else (0, 1, 2) if name[0][0] in "AB" else ():
            if i not in loaded:
                loaded.add(i)
                loads[i].wait()
        for need in messages[name][2]:
            if need in messages:
                arrival(need)
        start(name)

    names = [name for name in order if name in work]
    ahead = {}
    waiting = []
    for name in order:
        if name in work:
            ahead[name] = waiting
            waiting = []
        else:
            waiting.append(name)

    def before(name):
        previous = names.index(name) - 1
        if previous >= 0:
            kind, i, j = names[previous]
            if kind == "tile" and j in (0, 4):
                for n in LOOPS[i][0]:
                    at = pl.ds(mo(y * TOK, TOK), TOK)
                    if j == 0:
                        kv[n, at] = p[n, 0]
                    else:
                        qs[n, at] = p[n, 4, :, :HEAD]
        for item in ahead[name]:
            message(item)
        if name == names[-1]:
            for m, r in SPLIT:
                if m == 1:
                    arrival(("R", m, r, 0))
                    start(("F", m, r, 0))
        for need in work[name][1]:
            if need in messages:
                arrival(need)

    def loop(some, run, after=None):
        before(some[0])

        @pl.loop(0, len(some))
        def _(step):
            for k, name in enumerate(some):
                if k:
                    @pl.when(step == k)
                    def _():
                        before(name)
            run(step)
            for k, name in enumerate(some):
                if after and name in after:
                    @pl.when(step == k)
                    def _():
                        after[name]()

    def pick(values, step):
        value = jnp.int32(values[0])
        for k in range(1, len(values)):
            if values[k] != values[k - 1]:
                value = jnp.where(step >= k, values[k], value)
        return value

    for i, (blocks, tiles, _) in enumerate(LOOPS):
        def tile(step):
            j = pick(tiles, step)
            rows = t[blocks[0] : blocks[-1] + 1].reshape(len(blocks) * TOK, D)
            rows = jnp.dot(rows, w[:, pl.ds(mo(j * 256, 256), 256)], preferred_element_type=jnp.float32)
            rows = rows.astype(jnp.bfloat16).reshape(len(blocks), TOK, 256)
            for n, block in zip(blocks, rows):
                p[n, j] = block

        loop([("tile", i, j) for j in tiles], tile)

    pairs = [name for name in names if name[0] == "pair"]
    local = pltpu.make_async_copy(heads.at[0, pl.ds(mo(y * TOK, 16), TOK)], out.at[s], load_sem.at[4])

    for m in range(NX):
        high[m] = jnp.full((GROUP, HEAD), -1e30, jnp.float32)
        total[m] = jnp.zeros((GROUP, HEAD), jnp.float32)
        summed[m] = jnp.zeros((GROUP, HEAD), jnp.float32)

    def pair(step, which):
        m, n = (pick([some[which][i] for some in PAIRS], step) for i in (0, 1))
        a, b = (xs(pick([OFF[some[which][i]] for some in PAIRS], step)) for i in (0, 1))
        scale = HEAD**-0.5 * LOG2E
        base, keys = bias[a], bias[b]
        cuts = [(i * TOK, -(-(i + 1) * TOK // HEAD) * HEAD) for i in range(NY)]
        rows = [pl.ds(first, TOK) for first, _ in cuts]
        old = [(high[m, at], total[m, at], summed[m, at]) for at in rows]
        scores = [lax.dot_general(qs[m, at], kv[n, :width, :HEAD], (((1,), (1,)), ((), ())),
                                  preferred_element_type=jnp.float32) for at, (_, width) in zip(rows, cuts)]
        reach = jnp.clip(lax.broadcasted_iota(jnp.int32, (TOK, HEAD), 0) + (a - b) * TOK, -1, TOK - 1)
        lane = lax.broadcasted_iota(jnp.int32, (TOK, HEAD), 1)
        parts, tops = [], []
        for one, (first, width) in zip(scores, cuts):
            at = -(-first // HEAD) * HEAD
            shift = base[:, at : at + 1] - keys[:, :width]
            some = []
            for at in range(0, width, HEAD):
                part_of = one[:, at : at + HEAD] * scale + shift[:, at : at + HEAD]
                if at + HEAD > first:
                    part_of = jnp.where(lane + (at - first) <= reach, part_of, -1e30)
                some.append(part_of)
            parts.append(some)
            tops.append(jnp.max(fold(some, jnp.maximum), axis=1, keepdims=True))
        new = []
        for some, most, (before_, _, _), (_, width) in zip(parts, tops, old, cuts):
            top = jnp.maximum(before_, most)
            less = jnp.exp2(before_ - top)
            some = [jnp.exp2(one - top) for one in some]
            rounded = jnp.concatenate([one.astype(jnp.bfloat16) for one in some], axis=1)
            value = jnp.dot(rounded, kv[n, :width, HEAD:], preferred_element_type=jnp.float32)
            new.append((top, less, fold(some, jnp.add), value))
        for at, (top, less, low, value), (_, total_, summed_) in zip(rows, new, old):
            high[m, at] = top
            total[m, at] = total_ * less + low
            summed[m, at] = summed_ * less + value

    def finish(m):
        heads[m] = (summed[m] / jnp.sum(total[m], axis=1, keepdims=True)).astype(jnp.bfloat16)
        for r in (2, 1, 3, 0):
            if (m, r) in SPLIT:
                start(("R", m, r, 0))
        for r in (2, 1, 3, 0):
            if m or r:
                start(("O", m, r, 0))
            else:
                local.start()

    def run(step):
        pair(step, 0)
        pair(step, 1)

    loop(pairs, run, {pairs[k]: functools.partial(lambda ms: [finish(m) for m in ms], ms) for k, ms in DONE.items()})
    for m, r in SPLIT:
        if m != 1:
            arrival(("R", m, r, 0))
            start(("F", m, r, 0))
    for m in range(NX):
        for r in range(NY):
            if m or r:
                arrival(("O", m, r, 0))
    for m, r in SPLIT:
        arrival(("F", m, r, 0))
    local.wait()
    for name in started:
        source, target, _, who = regions(name)
        copy_of(name, source, target, who).wait_send()


def merge(heads, out, held, sem):
    come = [pltpu.make_async_copy(heads.at[i], held.at[i], sem.at[0, i]) for i in range(NX * NY)]
    go = [pltpu.make_async_copy(held.at[i], out.at[:, pl.ds(i * HEAD, HEAD)], sem.at[1, i]) for i in range(NX * NY)]
    for copy in come:
        copy.start()
    for one, other in zip(come, go):
        one.wait()
        other.start()
    for copy in go:
        copy.wait()


def body(tokens, query_weight, key_weight, value_weight, cum_gate):
    count = sum(len(m) for m in (weight_messages(0), weight_messages(1), token_messages(), *map(exchange_messages, range(NX))))
    any_space = pl.BlockSpec(memory_space=pl.ANY)
    vmem_space = pl.BlockSpec(memory_space=pltpu.VMEM)
    attended = pl.pallas_call(
        kernel,
        out_shape=jax.ShapeDtypeStruct((NX * NY, TOK, HEAD), jnp.bfloat16),
        in_specs=[any_space] * 4 + [vmem_space],
        out_specs=any_space,
        scratch_shapes=[
            pltpu.VMEM((D, NY * 3 * HEAD), jnp.bfloat16),
            pltpu.VMEM((NX, TOK, D), jnp.bfloat16),
            pltpu.VMEM((NX, 6, TOK, 2 * HEAD), jnp.bfloat16),
            pltpu.VMEM((NX, 2, HALF, 2 * HEAD), jnp.bfloat16),
            pltpu.VMEM((NX, 2, HALF, HEAD), jnp.bfloat16),
            pltpu.VMEM((NX, GROUP, 2 * HEAD), jnp.bfloat16),
            pltpu.VMEM((NX, GROUP, HEAD), jnp.bfloat16),
            pltpu.VMEM((NX, 1, GROUP), jnp.float32),
            pltpu.VMEM((NX, GROUP, HEAD), jnp.float32),
            pltpu.VMEM((NX, GROUP, HEAD), jnp.float32),
            pltpu.VMEM((NX, GROUP, HEAD), jnp.float32),
            pltpu.VMEM((NX, GROUP, HEAD), jnp.bfloat16),
            pltpu.VMEM((len(SPLIT), HALF, HEAD), jnp.bfloat16),
            pltpu.SemaphoreType.DMA((5,)),
            pltpu.SemaphoreType.DMA((count + NX * NY + 2 * len(SPLIT),)),
            pltpu.SemaphoreType.DMA((count + NX * NY + 2 * len(SPLIT),)),
        ],
        compiler_params=pltpu.CompilerParams(
            collective_id=0, has_side_effects=True, vmem_limit_bytes=60 * 1024 * 1024
        ),
        name="mixer",
    )(tokens[0], query_weight, key_weight, value_weight, cum_gate[0])
    merged = pl.pallas_call(
        merge,
        out_shape=jax.ShapeDtypeStruct((TOK, NX * NY * HEAD), jnp.bfloat16),
        in_specs=[any_space],
        out_specs=any_space,
        scratch_shapes=[pltpu.VMEM((NX * NY, TOK, HEAD), jnp.bfloat16), pltpu.SemaphoreType.DMA((2, NX * NY))],
        name="merge",
    )(attended)
    return merged[None]


def solution(mesh):
    in_specs = (
        P("dp", "sp", None),
        P("dp", "sp"),
        P("dp", "sp"),
        P("dp", "sp"),
        P("dp", "sp", None),
    )
    out_specs = P("dp", "sp", None)
    return jax.shard_map(body, mesh=mesh, in_specs=in_specs, out_specs=out_specs, check_vma=False)
```
